32 devices in a mesh: rep: 4 (over z), fs: 4 (over y, x), tp: 2 (over core).
Axes of the slice: x: 2, y: 2, z: 4, core: 2. Of those that a mesh axis runs over, the one named last changes fastest.
Arguments:
- inputs: bfloat16 [4096, 2048], P(('rep', 'fs', 'tp')), may hold values from -6 to 6
- out_grad: bfloat16 [4096, 2048], P(('rep', 'fs', 'tp')), may hold values from -6 to 6
- pre_act: bfloat16 [4096, 8192], P('rep', ('fs', 'tp')), may hold values from -6 to 6
- w_up: bfloat16 [2048, 8192], P('rep', ('fs', 'tp')), may hold values from -0.125 to 0.125
- w_down_t: bfloat16 [2048, 8192], P('rep', ('fs', 'tp')), may hold values from -0.0625 to 0.0625
Outputs:
- grad_in: bfloat16 [4096, 2048], P(('rep', 'fs', 'tp'))
- grad_up: float32 [2048, 8192], P('rep', ('fs', 'tp'))
- grad_down_t: float32 [2048, 8192], P('rep', ('fs', 'tp'))
The draws below stay inside these ranges and needn't reach their ends.
All inputs are finite; a program needn't handle non-finite values.
Results may differ from the reference program's by a relative error of at most 0.014.
Values may be sent and summed in bfloat16 or wider, within the bound.
A program may use at most 128 MiB of HBM per device.

```python
import jax
import jax.numpy as jnp
from jax import lax

D = 2048
FF = 8192
TOKENS = 4096
N_FS = 4
N_TP = 2


def with_spikes(entries, rng, source, target, shards_of, factor):
    owner, partner = [(jnp.arange(entries.shape[position]) // (entries.shape[position] // shards_of)).reshape([-1 if axis == position else 1 for axis in range(entries.ndim)]) for position in (source, target)]
    chosen = jax.random.permutation(rng, shards_of)[partner]
    strong = (owner == chosen) | (owner == (partner + shards_of // 2) % shards_of)
    return jnp.where(strong, factor * entries, entries)


def shard_levels(own_key, dims, cuts, low, top_value):
    level, own = 1.0, jax.random.fold_in(own_key, 6)
    for dim, shards_of in cuts:
        draws = jnp.exp(jax.random.uniform(jax.random.fold_in(own, dim), (shards_of,), jnp.float32, low / len(cuts), top_value / len(cuts)))
        level = level * jnp.repeat(draws, dims[dim] // shards_of).reshape([-1 if axis == dim else 1 for axis in range(len(dims))])
    return level


def noise(rng, extent, scale, most, cuts=(), dtype=jnp.bfloat16):
    factor_of = shard_levels(rng, extent, cuts, -0.22, 0.18) if cuts else 1.0
    values = jax.random.normal(rng, extent, jnp.float32) * scale * factor_of
    return jnp.minimum(jnp.maximum(values, -most), most).astype(dtype)


def noise_with(own_key, dims, spread, reach, pieces, heavy, kind=jnp.bfloat16):
    result = spread * jax.random.normal(own_key, dims, jnp.float32)
    if pieces:
        result = result * shard_levels(own_key, dims, pieces, -0.22, 0.18)
    return jnp.clip(with_spikes(result, jax.random.fold_in(own_key, 3), *heavy), -reach, reach).astype(kind)


def setup_inputs(seed: int = 0) -> dict:
    arg_keys = jax.random.split(jax.random.key(seed), 6)
    inputs = noise(arg_keys[0], (TOKENS, D), 1.0, 6.0, ((0, 32),))
    out_grad = noise_with(arg_keys[1], (TOKENS, D), 1.0, 6.0, ((0, 32),), (0, 1, 32, 2.75))
    pre_act = noise(arg_keys[2], (TOKENS, FF), 1.0, 6.0, ((0, 4), (1, 8)))
    w_up = noise(arg_keys[3], (D, FF), D ** -0.5, 0.125, ((0, 4), (1, 8)))
    w_down_t = noise(arg_keys[4], (D, FF), FF ** -0.5, 0.0625, ((0, 4), (1, 8)))
    return {"inputs": inputs, "out_grad": out_grad, "pre_act": pre_act, "w_up": w_up, "w_down_t": w_down_t}


def reference(inputs, out_grad, pre_act, w_up, w_down_t):
    pre_float = pre_act.astype(jnp.float32)
    linear = jnp.maximum(pre_float, 0.0)
    squared = (linear * linear).astype(jnp.bfloat16)
    grad_squared = jnp.dot(out_grad, w_down_t, preferred_element_type=jnp.float32)
    grad_pre = (grad_squared * 2.0 * linear).astype(jnp.bfloat16)
    factor = float(TOKENS) ** -0.5
    grad_down_t = jnp.dot(out_grad.T, squared, preferred_element_type=jnp.float32) * factor
    grad_up = jnp.dot(inputs.T, grad_pre, preferred_element_type=jnp.float32) * factor
    blocks = N_FS * N_TP
    width = FF // blocks
    total = jnp.zeros((inputs.shape[0], D), jnp.float32)
    for index in range(blocks):
        term = jnp.dot(grad_pre[:, index * width:(index + 1) * width], w_up[:, index * width:(index + 1) * width].T, preferred_element_type=jnp.float32)
        term = lax.optimization_barrier(term.astype(jnp.bfloat16))
        total = total + term.astype(jnp.float32)
    return total.astype(jnp.bfloat16), grad_up, grad_down_t
```

```python
import functools

import jax
import jax.numpy as jnp
from jax import lax
from jax.experimental import pallas as pl
from jax.experimental.pallas import tpu as pltpu
from jax.sharding import PartitionSpec as P

BF16 = jnp.bfloat16
F32 = jnp.float32


def kernel(
    n, n_fs, chunks, factor,
    x_ref, og_ref, pre_ref, wu_ref, wd_ref,
    gin_ref, gu_ref, gd_ref,
    rows_all, w_all, act, rs, tbuf, prec, frec, pre, total,
    zs, zr, xs, xr, cs, cr, ts, tr, fsend, frecv, ls,
):
    r, f, t = lax.axis_index("rep"), lax.axis_index("fs"), lax.axis_index("tp")
    tok, d_model = og_ref.shape
    shard, cols = wd_ref.shape
    crow = shard // chunks
    partner = {"tp": 1 - t}
    own_tokens = pl.ds(pl.multiple_of((f * 2 + t) * tok, tok), tok)
    own_rows_of = (og_ref, x_ref)
    own_w = (wd_ref, wu_ref)
    loads = [
        pltpu.make_async_copy(src, dst, ls.at[i])
        for i, (src, dst) in enumerate((
            (pre_ref, pre),
            (og_ref, rows_all.at[0, own_tokens, :]),
            (x_ref, rows_all.at[1, own_tokens, :]),
            (wd_ref, w_all.at[0, r]),
            (wu_ref, w_all.at[1, r]),
        ))
    ]
    peers = [None] + [{"fs": lax.rem(f + d, n_fs)} for d in range(1, n_fs)]
    ahead = ({"rep": lax.rem(r + 1, n)}, {"rep": lax.rem(r + n - 1, n)})
    depth = (r, n - 1 - r)
    after = (n - 1 - r, r)
    has_next = (r < n - 1, r > 0)

    barrier = pltpu.get_barrier_semaphore()
    for way in range(2):
        @pl.when(has_next[way])
        def _(way=way):
            pl.semaphore_signal(barrier, inc=1, device_id=ahead[way])
    for d in range(1, n_fs):
        pl.semaphore_signal(barrier, inc=1, device_id=peers[d])
    pl.semaphore_signal(barrier, inc=1, device_id=partner)
    pl.semaphore_wait(
        barrier, n_fs + jnp.where(r > 0, 1, 0) + jnp.where(r < n - 1, 1, 0)
    )

    def remote(src, dst, send, recv, target):
        return pltpu.make_async_remote_copy(
            src_ref=src, dst_ref=dst, send_sem=send, recv_sem=recv,
            device_id=target, device_id_type=pl.DeviceIdType.MESH,
        )

    def rows_of(q, ff, tt):
        return rows_all.at[
            q, pl.ds(pl.multiple_of((ff * 2 + tt) * tok, tok), tok), :
        ]

    def z_copy(p, way, k, j, src, dst):
        return remote(
            src, dst, zs.at[p, way, k, j], zr.at[p, way, k, j], ahead[way]
        )

    def rows_at(j):
        return pl.ds(pl.multiple_of(j * crow, crow), crow)

    def send_own(p, way):
        for j in range(chunks):
            z_copy(
                p, way, 0, j,
                own_w[p].at[rows_at(j), :], w_all.at[p, r, rows_at(j), :],
            ).start()

    def spread_start(q):
        own = own_rows_of[q]
        for d in range(1, n_fs):
            remote(
                own, rows_of(q, f, t), xs.at[q, d], xr.at[q, d], peers[d]
            ).start()
        remote(own, rows_of(q, f, t), cs.at[q, 0], cr.at[q, 0], partner).start()

    def spread_pass(q):
        for d in range(1, n_fs):
            src = rows_of(q, lax.rem(f + n_fs - d, n_fs), t)
            remote(src, src, xs.at[q, d], xr.at[q, d], peers[d]).wait()
            remote(src, src, cs.at[q, d], cr.at[q, d], partner).start()

    def spread_end(q):
        for d in range(n_fs):
            there = rows_of(q, lax.rem(f + n_fs - d, n_fs), 1 - t)
            remote(there, there, cs.at[q, d], cr.at[q, d], partner).wait()

    for way in range(2):
        @pl.when(has_next[way])
        def _(way=way):
            send_own(0, way)
    spread_start(0)
    for way in range(2):
        @pl.when(depth[way] == 0)
        def _(way=way):
            send_own(1, way)
    for load in loads:
        load.start()
    for load in loads:
        load.wait()
    tile = 2 * tok

    def square(i, _):
        at = pl.ds(pl.multiple_of(i * tile, tile), tile)
        linear = jnp.maximum(pre[at, :].astype(F32), 0.0)
        act[0, at, :] = (linear * linear).astype(BF16)
        return 0

    lax.fori_loop(0, n_fs, square, 0)

    def partial(p, s, j):
        at = pl.ds(pl.multiple_of(s * shard + j * crow, crow), crow)
        return lax.dot_general(
            rows_all[p, :, at], act[p], (((0,), (0,)), ((), ())),
            preferred_element_type=F32,
        ) * factor

    def own_partial(p):
        def body(j, _):
            total[p, rows_at(j), :] = partial(p, r, j)
            return 0

        lax.fori_loop(0, chunks, body, 0)

    def make_grad_pre(i, _):
        at = pl.ds(pl.multiple_of(i * tile, tile), tile)
        acc = jnp.zeros((tile, cols), F32)
        for s in range(n):
            acc += jnp.dot(
                rows_all[0, at, s * shard:(s + 1) * shard], w_all[0, s],
                preferred_element_type=F32,
            )
        linear = jnp.maximum(pre[at, :].astype(F32), 0.0)
        act[1, at, :] = (acc * 2.0 * linear).astype(BF16)
        return 0

    def cross(s):
        return remote(tbuf.at[s, 1 - t], prec.at[s], ts.at[s], tr.at[s], partner)

    def out_copy(s, d):
        rows = pl.ds(pl.multiple_of(lax.rem(f + d, n_fs) * tok, tok), tok)
        return remote(
            prec.at[s, rows, :], frec.at[s, d - 1],
            fsend.at[s, d], frecv.at[s, d], peers[d],
        )

    def block_term(s):
        def body(i, _):
            at = pl.ds(pl.multiple_of(i * tile, tile), tile)
            here = pl.ds(pl.multiple_of(i * tok, tok), tok)
            term = lax.dot_general(
                act[1, at, :], w_all[1, s], (((1,), (1,)), ((), ())),
                preferred_element_type=F32,
            ).astype(BF16)
            tbuf[s, 0, here, :] = term[:tok]
            tbuf[s, 1, here, :] = term[tok:]
            return 0

        lax.fori_loop(0, n_fs, body, 0)
        cross(s).start()

    def chip_sum(s):
        cross(s).wait()

        def body(i, _):
            here = pl.ds(pl.multiple_of(i * tok, tok), tok)
            prec[s, here, :] = (
                prec[s, here, :].astype(F32) + tbuf[s, t, here, :].astype(F32)
            ).astype(BF16)
            return 0

        lax.fori_loop(0, n_fs, body, 0)
        for d in range(1, n_fs):
            out_copy(s, d).start()

    def arrivals(step, way, j):
        d, h = depth[way], after[way]
        sign = 1 - 2 * way
        ag = step <= 2 * d
        p_ag = jnp.where(step > d, 1, 0)
        k = step - 1 - p_ag * d
        q = step - 2 * d - 1
        p_rs = jnp.where(q > h, 1, 0)
        i = q - p_rs * (h + 1) - jnp.where((d == 0) & (p_rs == 0), 1, 0)

        @pl.when(ag)
        def _():
            block = w_all.at[p_ag, r - sign * (1 + k), rows_at(j), :]
            z_copy(p_ag, way, k, j, block, block).wait_recv()

            @pl.when(h > 0)
            def _():
                z_copy(p_ag, way, k + 1, j, block, block).start()

        @pl.when(jnp.logical_not(ag) & (i >= 0) & (i < h))
        def _():
            s = n - 1 - i if way == 0 else i
            term = partial(p_rs, s, j)
            block = rs.at[p_rs, way, s, rows_at(j), :]

            @pl.when(d > 0)
            def _():
                z_copy(p_rs, way, d + i, j, block, block).wait_recv()
                rs[p_rs, way, s, rows_at(j), :] = (
                    term + rs[p_rs, way, s, rows_at(j), :].astype(F32)
                ).astype(BF16)

            @pl.when(d == 0)
            def _():
                rs[p_rs, way, s, rows_at(j), :] = term.astype(BF16)

            z_copy(p_rs, way, d + i + 1, j, block, block).start()

        @pl.when(jnp.logical_not(ag) & (i == h) & (d > 0))
        def _():
            take_own(p_rs, way, j)

    def take_own(p, way, j):
        block = rs.at[p, way, r, rows_at(j), :]
        z_copy(p, way, n - 1, j, block, block).wait_recv()
        total[p, rows_at(j), :] += rs[p, way, r, rows_at(j), :].astype(F32)

    def term_step(s):
        d = jnp.where(s < r, r, n - 1 - r)
        distance = jnp.where(s < r, r - s, s - r)
        return jnp.where(s == r, n - 1, jnp.maximum(d + distance, n - 1))

    def one_step(step, _):
        def body(j, _):
            for way in range(2):
                arrivals(step, way, j)
            return 0

        lax.fori_loop(0, chunks, body, 0)
        for way in range(2):
            @pl.when((depth[way] == step) & has_next[way])
            def _(way=way):
                send_own(1, way)

        @pl.when(step == 1)
        def _():
            spread_pass(0)
            spread_end(0)
            spread_start(1)

        @pl.when(step == 2)
        def _():
            own_partial(0)

        @pl.when(step == n - 1)
        def _():
            spread_pass(1)
            lax.fori_loop(0, n_fs, make_grad_pre, 0)
            spread_end(1)

        @pl.when(step == n + 1)
        def _():
            own_partial(1)

        def terms(s, _):
            @pl.when(term_step(s) == step)
            def _():
                block_term(s)

            @pl.when(term_step(s) + 1 == step)
            def _():
                chip_sum(s)
            return 0

        lax.fori_loop(0, n, terms, 0)
        return 0

    lax.fori_loop(1, 2 * n, one_step, 0)
    gd_ref[...] = total[0].astype(gd_ref.dtype)

    def last(j, _):
        for way in range(2):
            @pl.when(depth[way] > 0)
            def _(way=way):
                take_own(1, way, j)
        gu_ref[rows_at(j), :] = total[1, rows_at(j), :].astype(gu_ref.dtype)
        return 0

    lax.fori_loop(0, chunks - 1, last, 0)
    own_rows = pl.ds(pl.multiple_of(f * tok, tok), tok)
    for s in range(n):
        acc = prec[s, own_rows, :].astype(F32)
        for d in range(1, n_fs):
            out_copy(s, d).wait()
            acc += frec[s, d - 1].astype(F32)
        gin_ref[:, s * shard:(s + 1) * shard] = acc.astype(BF16)
    for way in range(2):
        @pl.when(has_next[way])
        def _(way=way):
            def body(k, _):
                for p in range(2):
                    for j in range(chunks):
                        block = rs.at[0, 0, 0, rows_at(j), :]
                        z_copy(p, way, k, j, block, block).wait_send()
                return 0

            lax.fori_loop(0, n, body, 0)
    lax.fori_loop(chunks - 1, chunks, last, 0)


def on_device(n, n_fs, inputs, out_grad, pre_act, w_up, w_down_t):
    tok, d_model = inputs.shape
    group, cols = pre_act.shape
    shard = w_up.shape[0]
    chunks = max(1, shard // 128)
    factor = float(group * n) ** -0.5
    dma = pltpu.SemaphoreType.DMA
    vmem = pl.BlockSpec(memory_space=pltpu.VMEM)
    grad_in, grad_up, grad_down_t = pl.pallas_call(
        functools.partial(kernel, n, n_fs, chunks, factor),
        out_shape=(
            jax.ShapeDtypeStruct((tok, d_model), BF16),
            jax.ShapeDtypeStruct((shard, cols), BF16),
            jax.ShapeDtypeStruct((shard, cols), BF16),
        ),
        in_specs=[pl.BlockSpec(memory_space=pl.ANY)] * 5,
        out_specs=(vmem,) * 3,
        scratch_shapes=[
            pltpu.VMEM((2, group, d_model), BF16),
            pltpu.VMEM((2, n, shard, cols), BF16),
            pltpu.VMEM((2, group, cols), BF16),
            pltpu.VMEM((2, 2, n, shard, cols), BF16),
            pltpu.VMEM((n, 2, n_fs * tok, shard), BF16),
            pltpu.VMEM((n, n_fs * tok, shard), BF16),
            pltpu.VMEM((n, n_fs - 1, tok, shard), BF16),
            pltpu.VMEM((group, cols), BF16),
            pltpu.VMEM((2, shard, cols), F32),
            dma((2, 2, n, chunks)),
            dma((2, 2, n, chunks)),
            dma((2, n_fs)),
            dma((2, n_fs)),
            dma((2, n_fs)),
            dma((2, n_fs)),
            dma((n,)),
            dma((n,)),
            dma((n, n_fs)),
            dma((n, n_fs)),
            dma((5,)),
        ],
        compiler_params=pltpu.CompilerParams(
            collective_id=0, has_side_effects=True, vmem_limit_bytes=67043328
        ),
    )(inputs, out_grad, pre_act, w_up, w_down_t)
    return grad_in, grad_up.astype(F32), grad_down_t.astype(F32)


def solution(mesh):
    rows = P(("rep", "fs", "tp"), None)
    blocks = P("rep", ("fs", "tp"))
    return jax.shard_map(
        functools.partial(on_device, mesh.shape["rep"], mesh.shape["fs"]),
        mesh=mesh,
        in_specs=(rows, rows, blocks, blocks, blocks),
        out_specs=(rows, blocks, blocks),
        check_vma=False,
    )
```

```python
import functools

import jax
import jax.numpy as jnp
from jax import lax
from jax.experimental import pallas as pl
from jax.experimental.pallas import tpu as pltpu
from jax.sharding import PartitionSpec as P

BF16 = jnp.bfloat16
F32 = jnp.float32


def kernel(
    n, n_fs, chunks, factor,
    x_ref, og_ref, pre_ref, wu_ref, wd_ref,
    gin_ref, gu_ref, gd_ref,
    rows_all, w_all, act, rs, tbuf, prec, frec, pre,
    zs, zr, xs, xr, cs, cr, ts, tr, fsend, frecv, ls,
):
    r, f, t = lax.axis_index("rep"), lax.axis_index("fs"), lax.axis_index("tp")
    tok, d_model = og_ref.shape
    shard, cols = wd_ref.shape
    crow = shard // chunks
    partner = {"tp": 1 - t}
    own_tokens = pl.ds(pl.multiple_of((f * 2 + t) * tok, tok), tok)
    totals = (gd_ref, gu_ref)
    loads = [
        pltpu.make_async_copy(src, dst, ls.at[i])
        for i, (src, dst) in enumerate((
            (wd_ref, w_all.at[0, r]),
            (og_ref, rows_all.at[0, own_tokens, :]),
            (wu_ref, w_all.at[1, r]),
            (pre_ref, pre),
            (x_ref, rows_all.at[1, own_tokens, :]),
        ))
    ]
    for load in loads:
        load.start()
    peers = [None] + [{"fs": lax.rem(f + d, n_fs)} for d in range(1, n_fs)]
    ahead = ({"rep": lax.rem(r + 1, n)}, {"rep": lax.rem(r + n - 1, n)})
    depth = (r, n - 1 - r)
    after = (n - 1 - r, r)
    has_next = (r < n - 1, r > 0)

    barrier = pltpu.get_barrier_semaphore()
    for way in range(2):
        @pl.when(has_next[way])
        def _(way=way):
            pl.semaphore_signal(barrier, inc=1, device_id=ahead[way])
    for d in range(1, n_fs):
        pl.semaphore_signal(barrier, inc=1, device_id=peers[d])
    pl.semaphore_signal(barrier, inc=1, device_id=partner)
    for load in loads[:3]:
        load.wait()
    pl.semaphore_wait(
        barrier, n_fs + jnp.where(r > 0, 1, 0) + jnp.where(r < n - 1, 1, 0)
    )

    def remote(src, dst, send, recv, target):
        return pltpu.make_async_remote_copy(
            src_ref=src, dst_ref=dst, send_sem=send, recv_sem=recv,
            device_id=target, device_id_type=pl.DeviceIdType.MESH,
        )

    def rows_of(q, ff, tt):
        return rows_all.at[
            q, pl.ds(pl.multiple_of((ff * 2 + tt) * tok, tok), tok), :
        ]

    def z_copy(p, way, k, j, src, dst):
        return remote(
            src, dst, zs.at[p, way, k, j], zr.at[p, way, k, j], ahead[way]
        )

    def rows_at(j):
        return pl.ds(pl.multiple_of(j * crow, crow), crow)

    def send_own(p, way):
        for j in range(chunks):
            block = w_all.at[p, r, rows_at(j), :]
            z_copy(p, way, 0, j, block, block).start()

    def spread_start(q):
        own = rows_of(q, f, t)
        for d in range(1, n_fs):
            remote(
                own, own, xs.at[q, d], xr.at[q, d], peers[d]
            ).start()
        remote(own, own, cs.at[q, 0], cr.at[q, 0], partner).start()

    def spread_pass(q):
        for d in range(1, n_fs):
            src = rows_of(q, lax.rem(f + n_fs - d, n_fs), t)
            remote(src, src, xs.at[q, d], xr.at[q, d], peers[d]).wait()
            remote(src, src, cs.at[q, d], cr.at[q, d], partner).start()

    def spread_end(q):
        for d in range(n_fs):
            there = rows_of(q, lax.rem(f + n_fs - d, n_fs), 1 - t)
            remote(there, there, cs.at[q, d], cr.at[q, d], partner).wait()

    for way in range(2):
        @pl.when(has_next[way])
        def _(way=way):
            send_own(0, way)
    spread_start(0)
    for way in range(2):
        @pl.when(depth[way] == 0)
        def _(way=way):
            send_own(1, way)
    for load in loads[3:]:
        load.wait()
    tile = 2 * tok

    def square(i, _):
        at = pl.ds(pl.multiple_of(i * tile, tile), tile)
        linear = jnp.maximum(pre[at, :].astype(F32), 0.0)
        act[0, at, :] = (linear * linear).astype(BF16)
        return 0

    lax.fori_loop(0, n_fs, square, 0)

    def partial(p, s, j):
        at = pl.ds(pl.multiple_of(s * shard + j * crow, crow), crow)
        return lax.dot_general(
            rows_all[p, :, at], act[p], (((0,), (0,)), ((), ())),
            preferred_element_type=F32,
        ) * factor

    def own_partial(p):
        def body(j, _):
            totals[p][rows_at(j), :] = partial(p, r, j)
            return 0

        lax.fori_loop(0, chunks, body, 0)

    def make_grad_pre(i, _):
        at = pl.ds(pl.multiple_of(i * tile, tile), tile)
        acc = jnp.zeros((tile, cols), F32)
        for s in range(n):
            acc += jnp.dot(
                rows_all[0, at, s * shard:(s + 1) * shard], w_all[0, s],
                preferred_element_type=F32,
            )
        linear = jnp.maximum(pre[at, :].astype(F32), 0.0)
        act[1, at, :] = (acc * 2.0 * linear).astype(BF16)
        return 0

    def cross(s):
        return remote(tbuf.at[s, 1 - t], prec.at[s], ts.at[s], tr.at[s], partner)

    def out_copy(s, d):
        rows = pl.ds(pl.multiple_of(lax.rem(f + d, n_fs) * tok, tok), tok)
        return remote(
            prec.at[s, rows, :], frec.at[s, d - 1],
            fsend.at[s, d], frecv.at[s, d], peers[d],
        )

    def block_term(s):
        def body(i, _):
            at = pl.ds(pl.multiple_of(i * tile, tile), tile)
            here = pl.ds(pl.multiple_of(i * tok, tok), tok)
            term = lax.dot_general(
                act[1, at, :], w_all[1, s], (((1,), (1,)), ((), ())),
                preferred_element_type=F32,
            ).astype(BF16)
            tbuf[s, 0, here, :] = term[:tok]
            tbuf[s, 1, here, :] = term[tok:]
            return 0

        lax.fori_loop(0, n_fs, body, 0)
        cross(s).start()

    def chip_sum(s):
        cross(s).wait()

        def body(i, _):
            here = pl.ds(pl.multiple_of(i * tok, tok), tok)
            prec[s, here, :] = (
                prec[s, here, :].astype(F32) + tbuf[s, t, here, :].astype(F32)
            ).astype(BF16)
            return 0

        lax.fori_loop(0, n_fs, body, 0)
        for d in range(1, n_fs):
            out_copy(s, d).start()

    def arrivals(step, way, j):
        d, h = depth[way], after[way]
        sign = 1 - 2 * way
        ag = step <= 2 * d
        p_ag = jnp.where(step > d, 1, 0)
        k = step - 1 - p_ag * d
        q = step - 2 * d - 1
        p_rs = jnp.where(q > h, 1, 0)
        i = q - p_rs * (h + 1) - jnp.where((d == 0) & (p_rs == 0), 1, 0)

        @pl.when(ag)
        def _():
            block = w_all.at[p_ag, r - sign * (1 + k), rows_at(j), :]
            z_copy(p_ag, way, k, j, block, block).wait_recv()

            @pl.when(h > 0)
            def _():
                z_copy(p_ag, way, k + 1, j, block, block).start()

        @pl.when(jnp.logical_not(ag) & (i >= 0) & (i < h))
        def _():
            s = n - 1 - i if way == 0 else i
            term = partial(p_rs, s, j)
            block = rs.at[p_rs, way, s, rows_at(j), :]

            @pl.when(d > 0)
            def _():
                z_copy(p_rs, way, d + i, j, block, block).wait_recv()
                rs[p_rs, way, s, rows_at(j), :] = (
                    term + rs[p_rs, way, s, rows_at(j), :].astype(F32)
                ).astype(BF16)

            @pl.when(d == 0)
            def _():
                rs[p_rs, way, s, rows_at(j), :] = term.astype(BF16)

            z_copy(p_rs, way, d + i + 1, j, block, block).start()

        @pl.when(jnp.logical_not(ag) & (i == h) & (d > 0))
        def _():
            take_own(0, way, j)

    def take_own(p, way, j):
        block = rs.at[p, way, r, rows_at(j), :]
        z_copy(p, way, n - 1, j, block, block).wait_recv()
        totals[p][rows_at(j), :] += rs[p, way, r, rows_at(j), :].astype(F32)

    def term_step(s):
        d = jnp.where(s < r, r, n - 1 - r)
        distance = jnp.where(s < r, r - s, s - r)
        return jnp.where(s == r, n - 1, jnp.maximum(d + distance, n - 1))

    def one_step(step, _):
        def body(j, _):
            for way in range(2):
                arrivals(step, way, j)
            return 0

        lax.fori_loop(0, chunks, body, 0)
        for way in range(2):
            @pl.when((depth[way] == step) & has_next[way])
            def _(way=way):
                send_own(1, way)

        @pl.when(step == 1)
        def _():
            spread_pass(0)
            spread_end(0)
            spread_start(1)

        @pl.when(step == 2)
        def _():
            own_partial(0)

        @pl.when(step == n - 1)
        def _():
            spread_pass(1)
            lax.fori_loop(0, n_fs, make_grad_pre, 0)
            spread_end(1)

        @pl.when(step == n + 1)
        def _():
            own_partial(1)

        def terms(s, _):
            @pl.when(term_step(s) == step)
            def _():
                block_term(s)

            @pl.when(term_step(s) + 1 == step)
            def _():
                chip_sum(s)
            return 0

        lax.fori_loop(0, n, terms, 0)
        return 0

    lax.fori_loop(1, 2 * n, one_step, 0)

    def last(j, _):
        for way in range(2):
            @pl.when(depth[way] > 0)
            def _(way=way):
                take_own(1, way, j)
        return 0

    lax.fori_loop(0, chunks - 1, last, 0)
    own_rows = pl.ds(pl.multiple_of(f * tok, tok), tok)
    for s in range(n):
        acc = prec[s, own_rows, :].astype(F32)
        for d in range(1, n_fs):
            out_copy(s, d).wait()
            acc += frec[s, d - 1].astype(F32)
        gin_ref[:, s * shard:(s + 1) * shard] = acc.astype(BF16)
    for way in range(2):
        @pl.when(has_next[way])
        def _(way=way):
            def body(k, _):
                for p in range(2):
                    for j in range(chunks):
                        block = rs.at[0, 0, 0, rows_at(j), :]
                        z_copy(p, way, k, j, block, block).wait_send()
                return 0

            lax.fori_loop(0, n, body, 0)
    lax.fori_loop(chunks - 1, chunks, last, 0)


def write_out(*refs):
    copies = [
        pltpu.make_async_copy(refs[i], refs[3 + i], refs[6].at[i]) for i in range(3)
    ]
    for copy in copies:
        copy.start()
    for copy in copies:
        copy.wait()


def on_device(n, n_fs, inputs, out_grad, pre_act, w_up, w_down_t):
    tok, d_model = inputs.shape
    group, cols = pre_act.shape
    shard = w_up.shape[0]
    chunks = max(1, shard // 128)
    factor = float(group * n) ** -0.5
    dma = pltpu.SemaphoreType.DMA
    vmem = pl.BlockSpec(memory_space=pltpu.VMEM)
    results = pl.pallas_call(
        functools.partial(kernel, n, n_fs, chunks, factor),
        out_shape=(
            pltpu.VMEM((tok, d_model), BF16),
            pltpu.VMEM((shard, cols), F32),
            pltpu.VMEM((shard, cols), F32),
        ),
        in_specs=[pl.BlockSpec(memory_space=pl.ANY)] * 5,
        out_specs=(vmem,) * 3,
        scratch_shapes=[
            pltpu.VMEM((2, group, d_model), BF16),
            pltpu.VMEM((2, n, shard, cols), BF16),
            pltpu.VMEM((2, group, cols), BF16),
            pltpu.VMEM((2, 2, n, shard, cols), BF16),
            pltpu.VMEM((n, 2, n_fs * tok, shard), BF16),
            pltpu.VMEM((n, n_fs * tok, shard), BF16),
            pltpu.VMEM((n, n_fs - 1, tok, shard), BF16),
            pltpu.VMEM((group, cols), BF16),
            dma((2, 2, n, chunks)),
            dma((2, 2, n, chunks)),
            dma((2, n_fs)),
            dma((2, n_fs)),
            dma((2, n_fs)),
            dma((2, n_fs)),
            dma((n,)),
            dma((n,)),
            dma((n, n_fs)),
            dma((n, n_fs)),
            dma((5,)),
        ],
        compiler_params=pltpu.CompilerParams(
            collective_id=0, has_side_effects=True, vmem_limit_bytes=56 * 2**20
        ),
    )(inputs, out_grad, pre_act, w_up, w_down_t)
    results = [pltpu.with_memory_space_constraint(a, pltpu.VMEM) for a in results]
    return pl.pallas_call(
        write_out,
        out_shape=[jax.ShapeDtypeStruct(a.shape, a.dtype) for a in results],
        in_specs=[vmem] * 3,
        out_specs=[pl.BlockSpec(memory_space=pl.ANY)] * 3,
        scratch_shapes=[dma((3,))],
        compiler_params=pltpu.CompilerParams(vmem_limit_bytes=2**20),
    )(*results)


def solution(mesh):
    rows = P(("rep", "fs", "tp"), None)
    blocks = P("rep", ("fs", "tp"))
    return jax.shard_map(
        functools.partial(on_device, mesh.shape["rep"], mesh.shape["fs"]),
        mesh=mesh,
        in_specs=(rows, rows, blocks, blocks, blocks),
        out_specs=(rows, blocks, blocks),
        check_vma=False,
    )
```

```python
import functools

import jax
import jax.numpy as jnp
from jax import lax
from jax.experimental import pallas as pl
from jax.experimental.pallas import tpu as pltpu
from jax.sharding import PartitionSpec as P

BF16 = jnp.bfloat16
F32 = jnp.float32


def kernel(
    n, n_fs, chunks, factor,
    x_ref, og_ref, pre_ref, wu_ref, wd_ref,
    gin_ref, gu_ref, gd_ref,
    rows_all, w_all, act, rs, tbuf, prec, frec, pre,
    zs, zr, xs, xr, cs, cr, ts, tr, fsend, frecv, ls,
):
    r, f, t = lax.axis_index("rep"), lax.axis_index("fs"), lax.axis_index("tp")
    tok, d_model = og_ref.shape
    shard, cols = wd_ref.shape
    crow = shard // chunks
    partner = {"tp": 1 - t}
    own_tokens = pl.ds(pl.multiple_of((f * 2 + t) * tok, tok), tok)
    totals = (gd_ref, gu_ref)
    loads = [
        pltpu.make_async_copy(src, dst, ls.at[i])
        for i, (src, dst) in enumerate((
            (wd_ref, w_all.at[0, r]),
            (og_ref, rows_all.at[0, own_tokens, :]),
            (wu_ref, w_all.at[1, r]),
            (pre_ref, pre),
            (x_ref, rows_all.at[1, own_tokens, :]),
        ))
    ]
    peers = [None] + [{"fs": lax.rem(f + d, n_fs)} for d in range(1, n_fs)]
    ahead = ({"rep": lax.rem(r + 1, n)}, {"rep": lax.rem(r + n - 1, n)})
    depth = (r, n - 1 - r)
    after = (n - 1 - r, r)
    has_next = (r < n - 1, r > 0)

    barrier = pltpu.get_barrier_semaphore()
    for way in range(2):
        @pl.when(has_next[way])
        def _(way=way):
            pl.semaphore_signal(barrier, inc=1, device_id=ahead[way])
    for d in range(1, n_fs):
        pl.semaphore_signal(barrier, inc=1, device_id=peers[d])
    pl.semaphore_signal(barrier, inc=1, device_id=partner)
    for load in loads:
        load.start()
    loads[0].wait()
    pl.semaphore_wait(
        barrier, n_fs + jnp.where(r > 0, 1, 0) + jnp.where(r < n - 1, 1, 0)
    )

    def remote(src, dst, send, recv, target):
        return pltpu.make_async_remote_copy(
            src_ref=src, dst_ref=dst, send_sem=send, recv_sem=recv,
            device_id=target, device_id_type=pl.DeviceIdType.MESH,
        )

    def rows_of(q, ff, tt):
        return rows_all.at[
            q, pl.ds(pl.multiple_of((ff * 2 + tt) * tok, tok), tok), :
        ]

    def z_copy(p, way, k, j, src, dst):
        return remote(
            src, dst, zs.at[way], zr.at[p, way, k, j], ahead[way]
        )

    def rows_at(j):
        return pl.ds(pl.multiple_of(j * crow, crow), crow)

    def send_own(p, way):
        for j in range(chunks):
            block = w_all.at[p, r, rows_at(j), :]
            z_copy(p, way, 0, j, block, block).start()

    def first_rows(q, count):
        return rows_all.at[q, pl.ds(0, count * tok), :]

    def spread(q, block, d):
        return remote(block, block, xs.at[q], xr.at[q], peers[d])

    def swap(q, block):
        return remote(block, block, cs.at[q], cr.at[q], partner)

    def spread_start(q):
        own = rows_of(q, f, t)
        for d in range(1, n_fs):
            spread(q, own, d).start()
        swap(q, own).start()

    def spread_pass(q):
        spread(q, first_rows(q, n_fs - 1), 1).wait_recv()
        for d in range(1, n_fs):
            swap(q, rows_of(q, lax.rem(f + d, n_fs), t)).start()

    def spread_end(q):
        swap(q, first_rows(q, n_fs)).wait_recv()

    for way in range(2):
        @pl.when(has_next[way])
        def _(way=way):
            send_own(0, way)
    loads[1].wait()
    spread_start(0)
    loads[2].wait()
    for way in range(2):
        @pl.when(depth[way] == 0)
        def _(way=way):
            send_own(1, way)
    for load in loads[3:]:
        load.wait()
    tile = 2 * tok

    def square(i, _):
        at = pl.ds(pl.multiple_of(i * tile, tile), tile)
        linear = jnp.maximum(pre[at, :].astype(F32), 0.0)
        act[0, at, :] = (linear * linear).astype(BF16)
        return 0

    lax.fori_loop(0, n_fs, square, 0)

    def partial(p, s, j):
        at = pl.ds(pl.multiple_of(s * shard + j * crow, crow), crow)
        return lax.dot_general(
            rows_all[p, :, at], act[p], (((0,), (0,)), ((), ())),
            preferred_element_type=F32,
        ) * factor

    def own_partial(p):
        def body(j, _):
            totals[p][rows_at(j), :] = partial(p, r, j)
            return 0

        lax.fori_loop(0, chunks, body, 0)

    def make_grad_pre(i, _):
        at = pl.ds(pl.multiple_of(i * tile, tile), tile)
        acc = jnp.zeros((tile, cols), F32)
        for s in range(n):
            acc += jnp.dot(
                rows_all[0, at, s * shard:(s + 1) * shard], w_all[0, s],
                preferred_element_type=F32,
            )
        linear = jnp.maximum(pre[at, :].astype(F32), 0.0)
        act[1, at, :] = (acc * 2.0 * linear).astype(BF16)
        return 0

    def cross(s):
        return remote(tbuf.at[s, 1 - t], prec.at[s], ts, tr.at[s], partner)

    def out_copy(s, d):
        rows = pl.ds(pl.multiple_of(lax.rem(f + d, n_fs) * tok, tok), tok)
        return remote(
            prec.at[s, rows, :], frec.at[s, d - 1],
            fsend, frecv, peers[d],
        )

    def block_term(s):
        def body(i, _):
            at = pl.ds(pl.multiple_of(i * tile, tile), tile)
            here = pl.ds(pl.multiple_of(i * tok, tok), tok)
            term = lax.dot_general(
                act[1, at, :], w_all[1, s], (((1,), (1,)), ((), ())),
                preferred_element_type=F32,
            ).astype(BF16)
            tbuf[s, 0, here, :] = term[:tok]
            tbuf[s, 1, here, :] = term[tok:]
            return 0

        lax.fori_loop(0, n_fs, body, 0)
        cross(s).start()

    def chip_sum(s):
        cross(s).wait_recv()

        def body(i, _):
            here = pl.ds(pl.multiple_of(i * tok, tok), tok)
            prec[s, here, :] = (
                prec[s, here, :].astype(F32) + tbuf[s, t, here, :].astype(F32)
            ).astype(BF16)
            return 0

        lax.fori_loop(0, n_fs, body, 0)
        for d in range(1, n_fs):
            out_copy(s, d).start()

    def arrivals(step, way, j):
        d, h = depth[way], after[way]
        sign = 1 - 2 * way
        ag = step <= 2 * d
        p_ag = jnp.where(step > d, 1, 0)
        k = step - 1 - p_ag * d
        q = step - 2 * d - 1
        p_rs = jnp.where(q > h, 1, 0)
        i = q - p_rs * (h + 1) - jnp.where((d == 0) & (p_rs == 0), 1, 0)

        @pl.when(ag)
        def _():
            block = w_all.at[p_ag, r - sign * (1 + k), rows_at(j), :]
            z_copy(p_ag, way, k, j, block, block).wait_recv()

            @pl.when(h > 0)
            def _():
                z_copy(p_ag, way, k + 1, j, block, block).start()

        @pl.when(jnp.logical_not(ag) & (i >= 0) & (i < h))
        def _():
            s = n - 1 - i if way == 0 else i
            term = partial(p_rs, s, j)
            block = rs.at[p_rs, way, s, rows_at(j), :]

            @pl.when(d > 0)
            def _():
                z_copy(p_rs, way, d + i, j, block, block).wait_recv()
                rs[p_rs, way, s, rows_at(j), :] = (
                    term + rs[p_rs, way, s, rows_at(j), :].astype(F32)
                ).astype(BF16)

            @pl.when(d == 0)
            def _():
                rs[p_rs, way, s, rows_at(j), :] = term.astype(BF16)

            z_copy(p_rs, way, d + i + 1, j, block, block).start()

        @pl.when(jnp.logical_not(ag) & (i == h) & (d > 0))
        def _():
            take_own(0, way, j)

    def take_own(p, way, j):
        block = rs.at[p, way, r, rows_at(j), :]
        z_copy(p, way, n - 1, j, block, block).wait_recv()
        totals[p][rows_at(j), :] += rs[p, way, r, rows_at(j), :].astype(F32)

    def term_step(s):
        d = jnp.where(s < r, r, n - 1 - r)
        distance = jnp.where(s < r, r - s, s - r)
        return jnp.where(s == r, n - 1, jnp.maximum(d + distance, n - 1))

    def one_step(step, _):
        def body(j, _):
            for way in range(2):
                arrivals(step, way, j)
            return 0

        lax.fori_loop(0, chunks, body, 0)
        for way in range(2):
            @pl.when((depth[way] == step) & has_next[way])
            def _(way=way):
                send_own(1, way)

        @pl.when(step == 1)
        def _():
            spread_pass(0)
            spread_end(0)
            spread_start(1)

        @pl.when(step == 2)
        def _():
            own_partial(0)

        @pl.when(step == n - 1)
        def _():
            spread_pass(1)
            lax.fori_loop(0, n_fs, make_grad_pre, 0)
            spread_end(1)

        @pl.when(step == n + 1)
        def _():
            own_partial(1)

        def terms(s, _):
            @pl.when(term_step(s) == step)
            def _():
                block_term(s)

            @pl.when(term_step(s) + 1 == step)
            def _():
                chip_sum(s)
            return 0

        lax.fori_loop(0, n, terms, 0)
        return 0

    lax.fori_loop(1, 2 * n, one_step, 0)

    def last(j, _):
        for way in range(2):
            @pl.when(depth[way] > 0)
            def _(way=way):
                take_own(1, way, j)
        return 0

    lax.fori_loop(0, chunks - 1, last, 0)
    own_rows = pl.ds(pl.multiple_of(f * tok, tok), tok)
    remote(frec, frec, fsend, frecv, peers[1]).wait()
    for s in range(n):
        acc = prec[s, own_rows, :].astype(F32)
        for d in range(1, n_fs):
            acc += frec[s, d - 1].astype(F32)
        gin_ref[:, s * shard:(s + 1) * shard] = acc.astype(BF16)
    remote(prec, prec, ts, tr.at[0], partner).wait_send()
    for q in range(2):
        spread(q, first_rows(q, n_fs - 1), 1).wait_send()
        swap(q, first_rows(q, n_fs)).wait_send()
    for way in range(2):
        @pl.when(has_next[way])
        def _(way=way):
            remote(w_all, w_all, zs.at[way], zr.at[0, way, 0, 0], ahead[way]).wait_send()
    lax.fori_loop(chunks - 1, chunks, last, 0)


def write_out(*refs):
    copies = [
        pltpu.make_async_copy(refs[i], refs[3 + i], refs[6].at[i]) for i in range(3)
    ]
    for copy in copies:
        copy.start()
    for copy in copies:
        copy.wait()


def on_device(n, n_fs, inputs, out_grad, pre_act, w_up, w_down_t):
    tok, d_model = inputs.shape
    group, cols = pre_act.shape
    shard = w_up.shape[0]
    chunks = max(1, shard // 256)
    factor = float(group * n) ** -0.5
    dma = pltpu.SemaphoreType.DMA
    vmem = pl.BlockSpec(memory_space=pltpu.VMEM)
    results = pl.pallas_call(
        functools.partial(kernel, n, n_fs, chunks, factor),
        out_shape=(
            pltpu.VMEM((tok, d_model), BF16),
            pltpu.VMEM((shard, cols), F32),
            pltpu.VMEM((shard, cols), F32),
        ),
        in_specs=[pl.BlockSpec(memory_space=pl.ANY)] * 5,
        out_specs=(vmem,) * 3,
        scratch_shapes=[
            pltpu.VMEM((2, group, d_model), BF16),
            pltpu.VMEM((2, n, shard, cols), BF16),
            pltpu.VMEM((2, group, cols), BF16),
            pltpu.VMEM((2, 2, n, shard, cols), BF16),
            pltpu.VMEM((n, 2, n_fs * tok, shard), BF16),
            pltpu.VMEM((n, n_fs * tok, shard), BF16),
            pltpu.VMEM((n, n_fs - 1, tok, shard), BF16),
            pltpu.VMEM((group, cols), BF16),
            dma((2,)),
            dma((2, 2, n, chunks)),
            dma((2,)),
            dma((2,)),
            dma((2,)),
            dma((2,)),
            dma(()),
            dma((n,)),
            dma(()),
            dma(()),
            dma((5,)),
        ],
        compiler_params=pltpu.CompilerParams(
            collective_id=0, has_side_effects=True, vmem_limit_bytes=56 * 2**20
        ),
    )(inputs, out_grad, pre_act, w_up, w_down_t)
    results = [pltpu.with_memory_space_constraint(a, pltpu.VMEM) for a in results]
    return pl.pallas_call(
        write_out,
        out_shape=[jax.ShapeDtypeStruct(a.shape, a.dtype) for a in results],
        in_specs=[vmem] * 3,
        out_specs=[pl.BlockSpec(memory_space=pl.ANY)] * 3,
        scratch_shapes=[dma((3,))],
        compiler_params=pltpu.CompilerParams(vmem_limit_bytes=2**20),
    )(*results)


def solution(mesh):
    rows = P(("rep", "fs", "tp"), None)
    blocks = P("rep", ("fs", "tp"))
    return jax.shard_map(
        functools.partial(on_device, mesh.shape["rep"], mesh.shape["fs"]),
        mesh=mesh,
        in_specs=(rows, rows, blocks, blocks, blocks),
        out_specs=(rows, blocks, blocks),
        check_vma=False,
    )
```

```python
import functools

import jax
import jax.numpy as jnp
from jax import lax
from jax.experimental import pallas as pl
from jax.experimental.pallas import tpu as pltpu
from jax.sharding import PartitionSpec as P

BF16 = jnp.bfloat16
F32 = jnp.float32


def kernel(
    n, n_fs, chunks, factor,
    x_ref, og_ref, pre_ref, wu_ref, wd_ref,
    gin_ref, gu_ref, gd_ref,
    rows_all, w_all, act, rs, tbuf, prec, frec, pre,
    zs, zr, xs, xr, cs, cr, ts, tr, fsend, frecv, ls,
):
    r, f, t = lax.axis_index("rep"), lax.axis_index("fs"), lax.axis_index("tp")
    tok, d_model = og_ref.shape
    shard, cols = wd_ref.shape
    crow = shard // chunks
    partner = {"tp": 1 - t}
    half = tok // 2
    own_tokens = pl.ds(pl.multiple_of((f * 2 + t) * tok, tok), tok)
    totals = (gd_ref, gu_ref)
    loads = [
        pltpu.make_async_copy(src, dst, ls.at[i])
        for i, (src, dst) in enumerate((
            (wd_ref, w_all.at[0, r]),
            (og_ref, rows_all.at[0, own_tokens, :]),
            (wu_ref, w_all.at[1, r]),
            (pre_ref, pre),
            (x_ref, rows_all.at[1, own_tokens, :]),
        ))
    ]
    peer = [None, f + 1 - 2 * lax.rem(f, 2), lax.rem(f + 2, n_fs), n_fs - 1 - f]
    peers = [None] + [{"fs": peer[d]} for d in range(1, n_fs)]
    ahead = ({"rep": lax.rem(r + 1, n)}, {"rep": lax.rem(r + n - 1, n)})
    depth = (r, n - 1 - r)
    after = (n - 1 - r, r)
    has_next = (r < n - 1, r > 0)

    barrier = pltpu.get_barrier_semaphore()
    for way in range(2):
        @pl.when(has_next[way])
        def _(way=way):
            pl.semaphore_signal(barrier, inc=1, device_id=ahead[way])
    for d in (1, 2):
        pl.semaphore_signal(barrier, inc=1, device_id=peers[d])
    pl.semaphore_signal(barrier, inc=1, device_id=partner)
    for load in loads:
        load.start()
    loads[0].wait()
    pl.semaphore_wait(
        barrier, 3 + jnp.where(r > 0, 1, 0) + jnp.where(r < n - 1, 1, 0)
    )

    def remote(src, dst, send, recv, target):
        return pltpu.make_async_remote_copy(
            src_ref=src, dst_ref=dst, send_sem=send, recv_sem=recv,
            device_id=target, device_id_type=pl.DeviceIdType.MESH,
        )

    def rows_of(q, ff, tt):
        return rows_all.at[
            q, pl.ds(pl.multiple_of((ff * 2 + tt) * tok, tok), tok), :
        ]

    def z_copy(p, way, k, j, src, dst):
        return remote(
            src, dst, zs.at[way], zr.at[p, way, k, j], ahead[way]
        )

    def rows_at(j):
        return pl.ds(pl.multiple_of(j * crow, crow), crow)

    def send_own(p, way):
        for j in range(chunks):
            block = w_all.at[p, r, rows_at(j), :]
            z_copy(p, way, 0, j, block, block).start()

    def first_rows(q, count):
        return rows_all.at[q, pl.ds(0, count * tok), :]

    def half_rows(q, ff, side):
        at = (ff * 2 + t) * tok + side * half
        return rows_all.at[q, pl.ds(pl.multiple_of(at, half), half), :]

    def spread(q, block, d, stage):
        return remote(block, block, xs.at[q], xr.at[q, stage], peers[d])

    def swap(q, block):
        return remote(block, block, cs.at[q], cr.at[q], partner)

    def spread_start(q):
        own = rows_of(q, f, t)
        for d in (1, 2):
            spread(q, own, d, 0).start()
        swap(q, own).start()

    def spread_relay(q):
        spread(q, first_rows(q, 2), 1, 0).wait_recv()
        spread(q, half_rows(q, peer[2], 0), 1, 1).start()
        spread(q, half_rows(q, peer[1], 1), 2, 1).start()
        for d in (1, 2):
            swap(q, rows_of(q, peer[d], t)).start()

    def spread_pass(q):
        spread(q, first_rows(q, 1), 1, 1).wait_recv()
        swap(q, rows_of(q, peer[3], t)).start()

    def spread_end(q):
        swap(q, first_rows(q, n_fs)).wait_recv()

    def first_sends():
        for way in range(2):
            @pl.when(has_next[way])
            def _(way=way):
                send_own(0, way)

    first_sends()

    loads[1].wait()
    spread_start(0)
    for load in loads[2:]:
        load.wait()
    tile = 2 * tok

    def square(i, _):
        at = pl.ds(pl.multiple_of(i * tile, tile), tile)
        linear = jnp.maximum(pre[at, :].astype(F32), 0.0)
        act[0, at, :] = (linear * linear).astype(BF16)
        return 0

    lax.fori_loop(0, n_fs, square, 0)


    for way in range(2):
        @pl.when(depth[way] == 0)
        def _(way=way):
            send_own(1, way)

    def partial(p, s, j):
        at = pl.ds(pl.multiple_of(s * shard + j * crow, crow), crow)
        return lax.dot_general(
            rows_all[p, :, at], act[p], (((0,), (0,)), ((), ())),
            preferred_element_type=F32,
        ) * factor

    def own_partial(p):
        def body(j, _):
            totals[p][rows_at(j), :] = partial(p, r, j)
            return 0

        lax.fori_loop(0, chunks, body, 0)

    def make_grad_pre(i, _):
        at = pl.ds(pl.multiple_of(i * tile, tile), tile)
        acc = jnp.zeros((tile, cols), F32)
        for s in range(n):
            acc += jnp.dot(
                rows_all[0, at, s * shard:(s + 1) * shard], w_all[0, s],
                preferred_element_type=F32,
            )
        linear = jnp.maximum(pre[at, :].astype(F32), 0.0)
        act[1, at, :] = (acc * 2.0 * linear).astype(BF16)
        return 0

    def cross(s):
        return remote(tbuf.at[s, 1 - t], prec.at[s], ts, tr.at[s], partner)

    def out_copy(s, d):
        rows = pl.ds(pl.multiple_of(peer[d] * tok, tok), tok)
        return remote(
            prec.at[s, rows, :], frec.at[s, d - 1],
            fsend, frecv, peers[d],
        )

    def block_term(s):
        def body(i, _):
            at = pl.ds(pl.multiple_of(i * tile, tile), tile)
            here = pl.ds(pl.multiple_of(i * tok, tok), tok)
            term = lax.dot_general(
                act[1, at, :], w_all[1, s], (((1,), (1,)), ((), ())),
                preferred_element_type=F32,
            ).astype(BF16)
            tbuf[s, 0, here, :] = term[:tok]
            tbuf[s, 1, here, :] = term[tok:]
            return 0

        lax.fori_loop(0, n_fs, body, 0)
        cross(s).start()

    def chip_sum(s):
        cross(s).wait_recv()

        def body(i, _):
            here = pl.ds(pl.multiple_of(i * tok, tok), tok)
            prec[s, here, :] = (
                prec[s, here, :].astype(F32) + tbuf[s, t, here, :].astype(F32)
            ).astype(BF16)
            return 0

        lax.fori_loop(0, n_fs, body, 0)
        for d in range(1, n_fs):
            out_copy(s, d).start()

    def arrivals(step, way, j):
        d, h = depth[way], after[way]
        sign = 1 - 2 * way
        ag = step <= 2 * d
        p_ag = jnp.where(step > d, 1, 0)
        k = step - 1 - p_ag * d
        q = step - 2 * d - 1
        p_rs = jnp.where(q > h, 1, 0)
        i = q - p_rs * (h + 1) - jnp.where((d == 0) & (p_rs == 0), 1, 0)

        @pl.when(ag)
        def _():
            block = w_all.at[p_ag, r - sign * (1 + k), rows_at(j), :]
            z_copy(p_ag, way, k, j, block, block).wait_recv()

            @pl.when(h > 0)
            def _():
                z_copy(p_ag, way, k + 1, j, block, block).start()

        @pl.when(jnp.logical_not(ag) & (i >= 0) & (i < h))
        def _():
            s = n - 1 - i if way == 0 else i
            term = partial(p_rs, s, j)
            block = rs.at[p_rs, way, s, rows_at(j), :]

            @pl.when(d > 0)
            def _():
                z_copy(p_rs, way, d + i, j, block, block).wait_recv()
                rs[p_rs, way, s, rows_at(j), :] = (
                    term + rs[p_rs, way, s, rows_at(j), :].astype(F32)
                ).astype(BF16)

            @pl.when(d == 0)
            def _():
                rs[p_rs, way, s, rows_at(j), :] = term.astype(BF16)

            z_copy(p_rs, way, d + i + 1, j, block, block).start()

        @pl.when(jnp.logical_not(ag) & (i == h) & (d > 0))
        def _():
            take_own(0, way, j)

    def take_own(p, way, j):
        block = rs.at[p, way, r, rows_at(j), :]
        z_copy(p, way, n - 1, j, block, block).wait_recv()
        totals[p][rows_at(j), :] += rs[p, way, r, rows_at(j), :].astype(F32)

    def term_step(s):
        d = jnp.where(s < r, r, n - 1 - r)
        distance = jnp.where(s < r, r - s, s - r)
        return jnp.where(s == r, n - 1, jnp.maximum(d + distance, n - 1))

    def one_step(step, _):
        def body(j, _):
            for way in range(2):
                arrivals(step, way, j)

            @pl.when((step <= 2) & (j == 0))
            def _():
                spread_relay(step - 1)
            return 0

        lax.fori_loop(0, chunks, body, 0)
        for way in range(2):
            @pl.when((depth[way] == step) & has_next[way])
            def _(way=way):
                send_own(1, way)

        @pl.when(step == 1)
        def _():
            spread_start(1)
            spread_pass(0)
            spread_end(0)

        @pl.when(step == 2)
        def _():
            own_partial(0)

        @pl.when(step == n - 1)
        def _():
            spread_pass(1)
            lax.fori_loop(0, n_fs, make_grad_pre, 0)
            spread_end(1)

        @pl.when(step == n + 1)
        def _():
            own_partial(1)

        def terms(s, _):
            @pl.when(term_step(s) == step)
            def _():
                block_term(s)

            @pl.when(term_step(s) + 1 == step)
            def _():
                chip_sum(s)
            return 0

        lax.fori_loop(0, n, terms, 0)
        return 0

    lax.fori_loop(1, 2 * n, one_step, 0)

    def last(j, _):
        for way in range(2):
            @pl.when(depth[way] > 0)
            def _(way=way):
                take_own(1, way, j)
        return 0

    lax.fori_loop(0, chunks - 1, last, 0)
    own_rows = pl.ds(pl.multiple_of(f * tok, tok), tok)
    remote(frec, frec, fsend, frecv, peers[1]).wait()
    for s in range(n):
        acc = prec[s, own_rows, :].astype(F32)
        for d in range(1, n_fs):
            acc += frec[s, d - 1].astype(F32)
        gin_ref[:, s * shard:(s + 1) * shard] = acc.astype(BF16)
    remote(prec, prec, ts, tr.at[0], partner).wait_send()
    for q in range(2):
        spread(q, first_rows(q, n_fs - 1), 1, 0).wait_send()
        swap(q, first_rows(q, n_fs)).wait_send()
    for way in range(2):
        @pl.when(has_next[way])
        def _(way=way):
            remote(w_all, w_all, zs.at[way], zr.at[0, way, 0, 0], ahead[way]).wait_send()
    lax.fori_loop(chunks - 1, chunks, last, 0)


def write_out(*refs):
    copies = [
        pltpu.make_async_copy(refs[i], refs[3 + i], refs[6].at[i]) for i in range(3)
    ]
    for copy in copies:
        copy.start()
    for copy in copies:
        copy.wait()


def on_device(n, n_fs, inputs, out_grad, pre_act, w_up, w_down_t):
    tok, d_model = inputs.shape
    group, cols = pre_act.shape
    shard = w_up.shape[0]
    chunks = max(1, shard // 256)
    factor = float(group * n) ** -0.5
    dma = pltpu.SemaphoreType.DMA
    vmem = pl.BlockSpec(memory_space=pltpu.VMEM)
    results = pl.pallas_call(
        functools.partial(kernel, n, n_fs, chunks, factor),
        out_shape=(
            pltpu.VMEM((tok, d_model), BF16),
            pltpu.VMEM((shard, cols), F32),
            pltpu.VMEM((shard, cols), F32),
        ),
        in_specs=[pl.BlockSpec(memory_space=pl.ANY)] * 5,
        out_specs=(vmem,) * 3,
        scratch_shapes=[
            pltpu.VMEM((2, group, d_model), BF16),
            pltpu.VMEM((2, n, shard, cols), BF16),
            pltpu.VMEM((2, group, cols), BF16),
            pltpu.VMEM((2, 2, n, shard, cols), BF16),
            pltpu.VMEM((n, 2, n_fs * tok, shard), BF16),
            pltpu.VMEM((n, n_fs * tok, shard), BF16),
            pltpu.VMEM((n, n_fs - 1, tok, shard), BF16),
            pltpu.VMEM((group, cols), BF16),
            dma((2,)),
            dma((2, 2, n, chunks)),
            dma((2,)),
            dma((2, 2)),
            dma((2,)),
            dma((2,)),
            dma(()),
            dma((n,)),
            dma(()),
            dma(()),
            dma((5,)),
        ],
        compiler_params=pltpu.CompilerParams(
            collective_id=0, has_side_effects=True, vmem_limit_bytes=56 * 2**20
        ),
    )(inputs, out_grad, pre_act, w_up, w_down_t)
    results = [pltpu.with_memory_space_constraint(a, pltpu.VMEM) for a in results]
    return pl.pallas_call(
        write_out,
        out_shape=[jax.ShapeDtypeStruct(a.shape, a.dtype) for a in results],
        in_specs=[vmem] * 3,
        out_specs=[pl.BlockSpec(memory_space=pl.ANY)] * 3,
        scratch_shapes=[dma((3,))],
        compiler_params=pltpu.CompilerParams(vmem_limit_bytes=2**20),
    )(*results)


def solution(mesh):
    rows = P(("rep", "fs", "tp"), None)
    blocks = P("rep", ("fs", "tp"))
    return jax.shard_map(
        functools.partial(on_device, mesh.shape["rep"], mesh.shape["fs"]),
        mesh=mesh,
        in_specs=(rows, rows, blocks, blocks, blocks),
        out_specs=(rows, blocks, blocks),
        check_vma=False,
    )
```

```python
import functools

import jax
import jax.numpy as jnp
from jax import lax
from jax.experimental import pallas as pl
from jax.experimental.pallas import tpu as pltpu
from jax.sharding import PartitionSpec as P

BF16 = jnp.bfloat16
F32 = jnp.float32


def kernel(
    n, n_fs, chunks, factor,
    x_ref, og_ref, pre_ref, wu_ref, wd_ref,
    gin_ref, gu_ref, gd_ref,
    rows_all, w_all, act, rs, tbuf, prec, frec, pre,
    zs, zr, xs, xr, cs, cr, ts, tr, fsend, frecv, ls, ready,
):
    r, f, t = lax.axis_index("rep"), lax.axis_index("fs"), lax.axis_index("tp")
    tok, d_model = og_ref.shape
    shard, cols = wd_ref.shape
    crow = shard // chunks
    partner = {"tp": 1 - t}
    half = tok // 2
    own_tokens = pl.ds(pl.multiple_of((f * 2 + t) * tok, tok), tok)
    totals = (gd_ref, gu_ref)
    loads = [
        pltpu.make_async_copy(src, dst, ls.at[i])
        for i, (src, dst) in enumerate((
            (wd_ref, w_all.at[0, r]),
            (og_ref, rows_all.at[0, own_tokens, :]),
            (wu_ref, w_all.at[1, r]),
            (pre_ref, pre),
            (x_ref, rows_all.at[1, own_tokens, :]),
        ))
    ]
    peer = [None, f + 1 - 2 * lax.rem(f, 2), lax.rem(f + 2, n_fs), n_fs - 1 - f]
    peers = [None] + [{"fs": peer[d]} for d in range(1, n_fs)]
    ahead = ({"rep": lax.rem(r + 1, n)}, {"rep": lax.rem(r + n - 1, n)})
    depth = (r, n - 1 - r)
    after = (n - 1 - r, r)
    has_next = (r < n - 1, r > 0)

    barrier = pltpu.get_barrier_semaphore()
    for way in range(2):
        @pl.when(has_next[way])
        def _(way=way):
            pl.semaphore_signal(barrier, inc=1, device_id=ahead[way])
    inner = (f > 0) & (f < n_fs - 1)

    @pl.when(jnp.logical_not(inner))
    def _():
        for d in (1, 2):
            pl.semaphore_signal(barrier, inc=1, device_id=peers[d])

    @pl.when(t == 0)
    def _():
        pl.semaphore_signal(barrier, inc=1, device_id=partner)

    for load in loads:
        load.start()
    pl.semaphore_wait(
        barrier,
        jnp.where(r > 0, 1, 0) + jnp.where(r < n - 1, 1, 0)
        + jnp.where(inner, 2, 0) + t,
    )

    @pl.when(inner)
    def _():
        for d in (1, 2):
            pl.semaphore_signal(ready, inc=1, device_id=peers[d])

    @pl.when(t == 1)
    def _():
        pl.semaphore_signal(ready, inc=1, device_id=partner)

    loads[0].wait()

    def remote(src, dst, send, recv, target):
        return pltpu.make_async_remote_copy(
            src_ref=src, dst_ref=dst, send_sem=send, recv_sem=recv,
            device_id=target, device_id_type=pl.DeviceIdType.MESH,
        )

    def rows_of(q, ff, tt):
        return rows_all.at[
            q, pl.ds(pl.multiple_of((ff * 2 + tt) * tok, tok), tok), :
        ]

    def z_copy(p, way, k, j, src, dst):
        return remote(
            src, dst, zs.at[way], zr.at[p, way, k, j], ahead[way]
        )

    def rows_at(j):
        return pl.ds(pl.multiple_of(j * crow, crow), crow)

    def send_own(p, way, pieces=range(chunks)):
        for j in pieces:
            block = w_all.at[p, r, rows_at(j), :]
            z_copy(p, way, 0, j, block, block).start()

    def first_rows(q, count):
        return rows_all.at[q, pl.ds(0, count * tok), :]

    def half_rows(q, ff, side):
        at = (ff * 2 + t) * tok + side * half
        return rows_all.at[q, pl.ds(pl.multiple_of(at, half), half), :]

    def spread(q, block, d, stage):
        return remote(block, block, xs.at[q], xr.at[q, stage], peers[d])

    def swap(q, block):
        return remote(block, block, cs.at[q], cr.at[q], partner)

    def spread_start(q):
        own = rows_of(q, f, t)
        for d in (1, 2):
            spread(q, own, d, 0).start()
        swap(q, own).start()

    def spread_relay(q):
        spread(q, first_rows(q, 2), 1, 0).wait_recv()
        spread(q, half_rows(q, peer[2], 0), 1, 1).start()
        spread(q, half_rows(q, peer[1], 1), 2, 1).start()
        for d in (1, 2):
            swap(q, rows_of(q, peer[d], t)).start()

    def spread_pass(q):
        spread(q, first_rows(q, 1), 1, 1).wait_recv()
        swap(q, rows_of(q, peer[3], t)).start()

    def spread_end(q):
        swap(q, first_rows(q, n_fs)).wait_recv()

    def rest_of_first_sends():
        for way in range(2):
            @pl.when(has_next[way])
            def _(way=way):
                send_own(0, way, range(1, chunks))

            @pl.when(depth[way] == 0)
            def _(way=way):
                send_own(1, way)

    for way in range(2):
        @pl.when(has_next[way])
        def _(way=way):
            send_own(0, way, range(1))

    loads[1].wait()

    @pl.when(jnp.logical_not(inner) | (t == 0))
    def _():
        pl.semaphore_wait(ready, jnp.where(inner, 0, 2) + 1 - t)

    spread_start(0)
    loads[2].wait()

    @pl.when(t == 0)
    def _():
        rest_of_first_sends()

    for load in loads[3:]:
        load.wait()
    tile = 2 * tok

    def square(i, _):
        at = pl.ds(pl.multiple_of(i * tile, tile), tile)
        linear = jnp.maximum(pre[at, :].astype(F32), 0.0)
        act[0, at, :] = (linear * linear).astype(BF16)
        return 0

    lax.fori_loop(0, n_fs, square, 0)


    def partial(p, s, j):
        at = pl.ds(pl.multiple_of(s * shard + j * crow, crow), crow)
        return lax.dot_general(
            rows_all[p, :, at], act[p], (((0,), (0,)), ((), ())),
            preferred_element_type=F32,
        ) * factor

    def own_partial(p):
        def body(j, _):
            totals[p][rows_at(j), :] = partial(p, r, j)
            return 0

        lax.fori_loop(0, chunks, body, 0)

    def make_grad_pre(i, _):
        at = pl.ds(pl.multiple_of(i * tile, tile), tile)
        acc = jnp.zeros((tile, cols), F32)
        for s in range(n):
            acc += jnp.dot(
                rows_all[0, at, s * shard:(s + 1) * shard], w_all[0, s],
                preferred_element_type=F32,
            )
        linear = jnp.maximum(pre[at, :].astype(F32), 0.0)
        act[1, at, :] = (acc * 2.0 * linear).astype(BF16)
        return 0

    def cross(s):
        return remote(tbuf.at[s, 1 - t], prec.at[s], ts, tr.at[s], partner)

    def out_copy(s, d):
        rows = pl.ds(pl.multiple_of(peer[d] * tok, tok), tok)
        return remote(
            prec.at[s, rows, :], frec.at[s, d - 1],
            fsend, frecv, peers[d],
        )

    def block_term(s):
        def body(i, _):
            at = pl.ds(pl.multiple_of(i * tile, tile), tile)
            here = pl.ds(pl.multiple_of(i * tok, tok), tok)
            term = lax.dot_general(
                act[1, at, :], w_all[1, s], (((1,), (1,)), ((), ())),
                preferred_element_type=F32,
            ).astype(BF16)
            tbuf[s, 0, here, :] = term[:tok]
            tbuf[s, 1, here, :] = term[tok:]
            return 0

        lax.fori_loop(0, n_fs, body, 0)
        cross(s).start()

    def chip_sum(s):
        cross(s).wait_recv()

        def body(i, _):
            here = pl.ds(pl.multiple_of(i * tok, tok), tok)
            prec[s, here, :] = (
                prec[s, here, :].astype(F32) + tbuf[s, t, here, :].astype(F32)
            ).astype(BF16)
            return 0

        lax.fori_loop(0, n_fs, body, 0)
        for d in range(1, n_fs):
            out_copy(s, d).start()

    def arrivals(step, way, j):
        d, h = depth[way], after[way]
        sign = 1 - 2 * way
        ag = step <= 2 * d
        p_ag = jnp.where(step > d, 1, 0)
        k = step - 1 - p_ag * d
        q = step - 2 * d - 1
        p_rs = jnp.where(q > h, 1, 0)
        i = q - p_rs * (h + 1) - jnp.where((d == 0) & (p_rs == 0), 1, 0)

        @pl.when(ag)
        def _():
            block = w_all.at[p_ag, r - sign * (1 + k), rows_at(j), :]
            z_copy(p_ag, way, k, j, block, block).wait_recv()

            @pl.when(h > 0)
            def _():
                z_copy(p_ag, way, k + 1, j, block, block).start()

        @pl.when(jnp.logical_not(ag) & (i >= 0) & (i < h))
        def _():
            s = n - 1 - i if way == 0 else i
            term = partial(p_rs, s, j)
            block = rs.at[p_rs, way, s, rows_at(j), :]

            @pl.when(d > 0)
            def _():
                z_copy(p_rs, way, d + i, j, block, block).wait_recv()
                rs[p_rs, way, s, rows_at(j), :] = (
                    term + rs[p_rs, way, s, rows_at(j), :].astype(F32)
                ).astype(BF16)

            @pl.when(d == 0)
            def _():
                rs[p_rs, way, s, rows_at(j), :] = term.astype(BF16)

            z_copy(p_rs, way, d + i + 1, j, block, block).start()

        @pl.when(jnp.logical_not(ag) & (i == h) & (d > 0))
        def _():
            take_own(0, way, j)

    def take_own(p, way, j):
        block = rs.at[p, way, r, rows_at(j), :]
        z_copy(p, way, n - 1, j, block, block).wait_recv()
        totals[p][rows_at(j), :] += rs[p, way, r, rows_at(j), :].astype(F32)

    def term_step(s):
        d = jnp.where(s < r, r, n - 1 - r)
        distance = jnp.where(s < r, r - s, s - r)
        return jnp.where(s == r, n - 1, jnp.maximum(d + distance, n - 1))

    def one_step(step, _):
        def body(j, _):
            for way in range(2):
                arrivals(step, way, j)

            @pl.when((step <= 2) & (j == 0))
            def _():
                spread_relay(step - 1)

            @pl.when((step == 1) & (j == 0) & (t == 1))
            def _():
                rest_of_first_sends()
            return 0

        lax.fori_loop(0, chunks, body, 0)
        for way in range(2):
            @pl.when((depth[way] == step) & has_next[way])
            def _(way=way):
                send_own(1, way)

        @pl.when(step == 1)
        def _():
            spread_start(1)
            spread_pass(0)
            spread_end(0)

        @pl.when(step == 2)
        def _():
            own_partial(0)

        @pl.when(step == n - 1)
        def _():
            spread_pass(1)
            lax.fori_loop(0, n_fs, make_grad_pre, 0)
            spread_end(1)

        @pl.when(step == n + 1)
        def _():
            own_partial(1)

        def terms(s, _):
            @pl.when(term_step(s) == step)
            def _():
                block_term(s)

            @pl.when(term_step(s) + 1 == step)
            def _():
                chip_sum(s)
            return 0

        lax.fori_loop(0, n, terms, 0)
        return 0

    lax.fori_loop(1, 2 * n, one_step, 0)

    def last(j, _):
        for way in range(2):
            @pl.when(depth[way] > 0)
            def _(way=way):
                take_own(1, way, j)
        return 0

    lax.fori_loop(0, chunks - 1, last, 0)
    own_rows = pl.ds(pl.multiple_of(f * tok, tok), tok)
    remote(frec, frec, fsend, frecv, peers[1]).wait()
    for s in range(n):
        acc = prec[s, own_rows, :].astype(F32)
        for d in range(1, n_fs):
            acc += frec[s, d - 1].astype(F32)
        gin_ref[:, s * shard:(s + 1) * shard] = acc.astype(BF16)
    remote(prec, prec, ts, tr.at[0], partner).wait_send()
    for q in range(2):
        spread(q, first_rows(q, n_fs - 1), 1, 0).wait_send()
        swap(q, first_rows(q, n_fs)).wait_send()
    for way in range(2):
        @pl.when(has_next[way])
        def _(way=way):
            remote(w_all, w_all, zs.at[way], zr.at[0, way, 0, 0], ahead[way]).wait_send()
    lax.fori_loop(chunks - 1, chunks, last, 0)


def write_out(*refs):
    copies = [
        pltpu.make_async_copy(refs[i], refs[3 + i], refs[6].at[i]) for i in range(3)
    ]
    for copy in copies:
        copy.start()
    for copy in copies:
        copy.wait()


def on_device(n, n_fs, inputs, out_grad, pre_act, w_up, w_down_t):
    tok, d_model = inputs.shape
    group, cols = pre_act.shape
    shard = w_up.shape[0]
    chunks = max(1, shard // 256)
    factor = float(group * n) ** -0.5
    dma = pltpu.SemaphoreType.DMA
    vmem = pl.BlockSpec(memory_space=pltpu.VMEM)
    results = pl.pallas_call(
        functools.partial(kernel, n, n_fs, chunks, factor),
        out_shape=(
            pltpu.VMEM((tok, d_model), BF16),
            pltpu.VMEM((shard, cols), F32),
            pltpu.VMEM((shard, cols), F32),
        ),
        in_specs=[pl.BlockSpec(memory_space=pl.ANY)] * 5,
        out_specs=(vmem,) * 3,
        scratch_shapes=[
            pltpu.VMEM((2, group, d_model), BF16),
            pltpu.VMEM((2, n, shard, cols), BF16),
            pltpu.VMEM((2, group, cols), BF16),
            pltpu.VMEM((2, 2, n, shard, cols), BF16),
            pltpu.VMEM((n, 2, n_fs * tok, shard), BF16),
            pltpu.VMEM((n, n_fs * tok, shard), BF16),
            pltpu.VMEM((n, n_fs - 1, tok, shard), BF16),
            pltpu.VMEM((group, cols), BF16),
            dma((2,)),
            dma((2, 2, n, chunks)),
            dma((2,)),
            dma((2, 2)),
            dma((2,)),
            dma((2,)),
            dma(()),
            dma((n,)),
            dma(()),
            dma(()),
            dma((5,)),
            pltpu.SemaphoreType.REGULAR,
        ],
        compiler_params=pltpu.CompilerParams(
            collective_id=0, has_side_effects=True, vmem_limit_bytes=56 * 2**20
        ),
    )(inputs, out_grad, pre_act, w_up, w_down_t)
    results = [pltpu.with_memory_space_constraint(a, pltpu.VMEM) for a in results]
    return pl.pallas_call(
        write_out,
        out_shape=[jax.ShapeDtypeStruct(a.shape, a.dtype) for a in results],
        in_specs=[vmem] * 3,
        out_specs=[pl.BlockSpec(memory_space=pl.ANY)] * 3,
        scratch_shapes=[dma((3,))],
        compiler_params=pltpu.CompilerParams(vmem_limit_bytes=2**20),
    )(*results)


def solution(mesh):
    rows = P(("rep", "fs", "tp"), None)
    blocks = P("rep", ("fs", "tp"))
    return jax.shard_map(
        functools.partial(on_device, mesh.shape["rep"], mesh.shape["fs"]),
        mesh=mesh,
        in_specs=(rows, rows, blocks, blocks, blocks),
        out_specs=(rows, blocks, blocks),
        check_vma=False,
    )
```

```python
import functools

import jax
import jax.numpy as jnp
from jax import lax
from jax.experimental import pallas as pl
from jax.experimental.pallas import tpu as pltpu
from jax.sharding import PartitionSpec as P

BF16 = jnp.bfloat16
F32 = jnp.float32


def kernel(
    n, n_fs, chunks, factor,
    x_ref, og_ref, pre_ref, wu_ref, wd_ref,
    gin_ref, gu_ref, gd_ref,
    rows_all, w_all, act, rs, tbuf, prec, frec, pre,
    zs, z_last, fsend, frecv,
):
    r, f, t = lax.axis_index("rep"), lax.axis_index("fs"), lax.axis_index("tp")
    tok, d_model = og_ref.shape
    shard, cols = wd_ref.shape
    crow = shard // chunks
    partner = {"tp": 1 - t}
    half = tok // 2
    own_tokens = pl.ds(pl.multiple_of((f * 2 + t) * tok, tok), tok)
    totals = (gd_ref, gu_ref)
    peer = [None, f + 1 - 2 * lax.rem(f, 2), lax.rem(f + 2, n_fs), n_fs - 1 - f]
    peers = [None] + [{"fs": peer[d]} for d in range(1, n_fs)]
    ahead = ({"rep": lax.rem(r + 1, n)}, {"rep": lax.rem(r + n - 1, n)})
    depth = (r, n - 1 - r)
    after = (n - 1 - r, r)
    has_next = (r < n - 1, r > 0)

    def remote(src, dst, send, recv, target):
        return pltpu.make_async_remote_copy(
            src_ref=src, dst_ref=dst, send_sem=send, recv_sem=recv,
            device_id=target, device_id_type=pl.DeviceIdType.MESH,
        )

    def rows_at(j):
        return pl.ds(pl.multiple_of(j * crow, crow), crow)

    def z_final(way, s, j):
        block = rs.at[1, way, s, rows_at(j), :]
        return remote(block, block, zs.at[way], z_last.at[way, j], ahead[way])

    def all_but_last_step(zr, xs, xr, cs, cr, ts, tr, ls, ready):
        loads = [
            pltpu.make_async_copy(src, dst, ls.at[i])
            for i, (src, dst) in enumerate((
                (wd_ref, w_all.at[0, r]),
                (og_ref, rows_all.at[0, own_tokens, :]),
                (wu_ref, w_all.at[1, r]),
                (pre_ref, pre),
                (x_ref, rows_all.at[1, own_tokens, :]),
            ))
        ]
        barrier = pltpu.get_barrier_semaphore()
        for way in range(2):
            @pl.when(has_next[way])
            def _(way=way):
                pl.semaphore_signal(barrier, inc=1, device_id=ahead[way])
        inner = (f > 0) & (f < n_fs - 1)

        @pl.when(jnp.logical_not(inner))
        def _():
            for d in (1, 2):
                pl.semaphore_signal(barrier, inc=1, device_id=peers[d])

        @pl.when(t == 0)
        def _():
            pl.semaphore_signal(barrier, inc=1, device_id=partner)

        for load in loads:
            load.start()
        pl.semaphore_wait(
            barrier,
            jnp.where(r > 0, 1, 0) + jnp.where(r < n - 1, 1, 0)
            + jnp.where(inner, 2, 0) + t,
        )

        @pl.when(inner)
        def _():
            for d in (1, 2):
                pl.semaphore_signal(ready, inc=1, device_id=peers[d])

        @pl.when(t == 1)
        def _():
            pl.semaphore_signal(ready, inc=1, device_id=partner)

        loads[0].wait()

        def rows_of(q, ff, tt):
            return rows_all.at[
                q, pl.ds(pl.multiple_of((ff * 2 + tt) * tok, tok), tok), :
            ]

        def z_copy(p, way, k, j, src, dst):
            return remote(src, dst, zs.at[way], zr.at[p, way, k, j], ahead[way])

        def send_own(p, way, pieces=range(chunks)):
            for j in pieces:
                block = w_all.at[p, r, rows_at(j), :]
                z_copy(p, way, 0, j, block, block).start()

        def first_rows(q, count):
            return rows_all.at[q, pl.ds(0, count * tok), :]

        def half_rows(q, ff, side):
            at = (ff * 2 + t) * tok + side * half
            return rows_all.at[q, pl.ds(pl.multiple_of(at, half), half), :]

        def spread(q, block, d, stage):
            return remote(block, block, xs.at[q], xr.at[q, stage], peers[d])

        def swap(q, block):
            return remote(block, block, cs.at[q], cr.at[q], partner)

        def spread_start(q):
            own = rows_of(q, f, t)
            for d in (1, 2):
                spread(q, own, d, 0).start()
            swap(q, own).start()

        def spread_relay(q):
            spread(q, first_rows(q, 2), 1, 0).wait_recv()
            spread(q, half_rows(q, peer[2], 0), 1, 1).start()
            spread(q, half_rows(q, peer[1], 1), 2, 1).start()
            for d in (1, 2):
                swap(q, rows_of(q, peer[d], t)).start()

        def spread_pass(q):
            spread(q, first_rows(q, 1), 1, 1).wait_recv()
            swap(q, rows_of(q, peer[3], t)).start()

        def spread_end(q):
            swap(q, first_rows(q, n_fs)).wait_recv()

        def rest_of_first_sends():
            for way in range(2):
                @pl.when(has_next[way])
                def _(way=way):
                    send_own(0, way, range(1, chunks))

                @pl.when(depth[way] == 0)
                def _(way=way):
                    send_own(1, way)

        for way in range(2):
            @pl.when(has_next[way])
            def _(way=way):
                send_own(0, way, range(1))

        loads[1].wait()

        @pl.when(jnp.logical_not(inner) | (t == 0))
        def _():
            pl.semaphore_wait(ready, jnp.where(inner, 0, 2) + 1 - t)

        spread_start(0)
        loads[2].wait()

        @pl.when(t == 0)
        def _():
            rest_of_first_sends()

        for load in loads[3:]:
            load.wait()
        tile = 2 * tok

        def square(i, _):
            at = pl.ds(pl.multiple_of(i * tile, tile), tile)
            linear = jnp.maximum(pre[at, :].astype(F32), 0.0)
            act[0, at, :] = (linear * linear).astype(BF16)
            return 0

        lax.fori_loop(0, n_fs, square, 0)


        def partial(p, s, j):
            at = pl.ds(pl.multiple_of(s * shard + j * crow, crow), crow)
            return lax.dot_general(
                rows_all[p, :, at], act[p], (((0,), (0,)), ((), ())),
                preferred_element_type=F32,
            ) * factor

        def own_partial(p):
            def body(j, _):
                totals[p][rows_at(j), :] = partial(p, r, j)
                return 0

            lax.fori_loop(0, chunks, body, 0)

        def make_grad_pre(i, _):
            at = pl.ds(pl.multiple_of(i * tile, tile), tile)
            acc = jnp.zeros((tile, cols), F32)
            for s in range(n):
                acc += jnp.dot(
                    rows_all[0, at, s * shard:(s + 1) * shard], w_all[0, s],
                    preferred_element_type=F32,
                )
            linear = jnp.maximum(pre[at, :].astype(F32), 0.0)
            act[1, at, :] = (acc * 2.0 * linear).astype(BF16)
            return 0

        def cross(s):
            return remote(tbuf.at[s, 1 - t], prec.at[s], ts, tr.at[s], partner)

        def out_copy(s, d):
            rows = pl.ds(pl.multiple_of(peer[d] * tok, tok), tok)
            return remote(
                prec.at[s, rows, :], frec.at[s, d - 1],
                fsend, frecv, peers[d],
            )

        def block_term(s):
            def body(i, _):
                at = pl.ds(pl.multiple_of(i * tile, tile), tile)
                here = pl.ds(pl.multiple_of(i * tok, tok), tok)
                term = lax.dot_general(
                    act[1, at, :], w_all[1, s], (((1,), (1,)), ((), ())),
                    preferred_element_type=F32,
                ).astype(BF16)
                tbuf[s, 0, here, :] = term[:tok]
                tbuf[s, 1, here, :] = term[tok:]
                return 0

            lax.fori_loop(0, n_fs, body, 0)
            cross(s).start()

        def chip_sum(s):
            cross(s).wait_recv()

            def body(i, _):
                here = pl.ds(pl.multiple_of(i * tok, tok), tok)
                prec[s, here, :] = (
                    prec[s, here, :].astype(F32) + tbuf[s, t, here, :].astype(F32)
                ).astype(BF16)
                return 0

            lax.fori_loop(0, n_fs, body, 0)
            for d in range(1, n_fs):
                out_copy(s, d).start()

        def arrivals(step, way, j):
            d, h = depth[way], after[way]
            sign = 1 - 2 * way
            ag = step <= 2 * d
            p_ag = jnp.where(step > d, 1, 0)
            k = step - 1 - p_ag * d
            q = step - 2 * d - 1
            p_rs = jnp.where(q > h, 1, 0)
            i = q - p_rs * (h + 1) - jnp.where((d == 0) & (p_rs == 0), 1, 0)

            @pl.when(ag)
            def _():
                block = w_all.at[p_ag, r - sign * (1 + k), rows_at(j), :]
                z_copy(p_ag, way, k, j, block, block).wait_recv()

                @pl.when(h > 0)
                def _():
                    z_copy(p_ag, way, k + 1, j, block, block).start()

            @pl.when(jnp.logical_not(ag) & (i >= 0) & (i < h))
            def _():
                s = n - 1 - i if way == 0 else i
                term = partial(p_rs, s, j)
                block = rs.at[p_rs, way, s, rows_at(j), :]

                @pl.when(d > 0)
                def _():
                    z_copy(p_rs, way, d + i, j, block, block).wait_recv()
                    rs[p_rs, way, s, rows_at(j), :] = (
                        term + rs[p_rs, way, s, rows_at(j), :].astype(F32)
                    ).astype(BF16)

                @pl.when(d == 0)
                def _():
                    rs[p_rs, way, s, rows_at(j), :] = term.astype(BF16)

                final = (p_rs == 1) & (i == h - 1)

                @pl.when(final)
                def _():
                    z_final(way, s, j).start()

                @pl.when(jnp.logical_not(final))
                def _():
                    z_copy(p_rs, way, d + i + 1, j, block, block).start()

            @pl.when(jnp.logical_not(ag) & (i == h) & (d > 0))
            def _():
                block = rs.at[0, way, r, rows_at(j), :]
                z_copy(0, way, n - 1, j, block, block).wait_recv()
                gd_ref[rows_at(j), :] += rs[0, way, r, rows_at(j), :].astype(F32)

        def term_step(s):
            d = jnp.where(s < r, r, n - 1 - r)
            distance = jnp.where(s < r, r - s, s - r)
            return jnp.where(s == r, n - 1, jnp.maximum(d + distance, n - 1))

        def one_step(step, _):
            def body(j, _):
                for way in range(2):
                    arrivals(step, way, j)

                @pl.when((step <= 2) & (j == 0))
                def _():
                    spread_relay(step - 1)

                @pl.when((step == 1) & (j == 0) & (t == 1))
                def _():
                    rest_of_first_sends()
                return 0

            lax.fori_loop(0, chunks, body, 0)
            for way in range(2):
                @pl.when((depth[way] == step) & has_next[way])
                def _(way=way):
                    send_own(1, way)

            @pl.when(step == 1)
            def _():
                spread_start(1)
                spread_pass(0)
                spread_end(0)

            @pl.when(step == 2)
            def _():
                own_partial(0)

            @pl.when(step == n - 1)
            def _():
                spread_pass(1)
                lax.fori_loop(0, n_fs, make_grad_pre, 0)
                spread_end(1)

            @pl.when(step == n + 1)
            def _():
                own_partial(1)

            def terms(s, _):
                @pl.when(term_step(s) == step)
                def _():
                    block_term(s)

                @pl.when(term_step(s) + 1 == step)
                def _():
                    chip_sum(s)
                return 0

            lax.fori_loop(0, n, terms, 0)
            return 0

        lax.fori_loop(1, 2 * n, one_step, 0)
        remote(prec, prec, ts, tr.at[0], partner).wait_send()
        for q in range(2):
            spread(q, first_rows(q, n_fs - 1), 1, 0).wait_send()
            swap(q, first_rows(q, n_fs)).wait_send()

    dma = pltpu.SemaphoreType.DMA
    pl.run_scoped(
        all_but_last_step,
        dma((2, 2, n, chunks)), dma((2,)), dma((2, 2)), dma((2,)), dma((2,)),
        dma(()), dma((n,)), dma((5,)), pltpu.SemaphoreType.REGULAR,
    )

    def last(j, _):
        for way in range(2):
            @pl.when(depth[way] > 0)
            def _(way=way):
                z_final(way, r, j).wait_recv()
                gu_ref[rows_at(j), :] += rs[1, way, r, rows_at(j), :].astype(F32)
        return 0

    lax.fori_loop(0, chunks - 1, last, 0)
    own_rows = pl.ds(pl.multiple_of(f * tok, tok), tok)
    remote(frec, frec, fsend, frecv, peers[1]).wait()
    for s in range(n):
        acc = prec[s, own_rows, :].astype(F32)
        for d in range(1, n_fs):
            acc += frec[s, d - 1].astype(F32)
        gin_ref[:, s * shard:(s + 1) * shard] = acc.astype(BF16)
    for way in range(2):
        @pl.when(has_next[way])
        def _(way=way):
            remote(w_all, w_all, zs.at[way], z_last.at[way, 0], ahead[way]).wait_send()
    lax.fori_loop(chunks - 1, chunks, last, 0)


def write_out(*refs):
    copies = [
        pltpu.make_async_copy(refs[i], refs[3 + i], refs[6].at[i]) for i in range(3)
    ]
    for copy in copies:
        copy.start()
    for copy in copies:
        copy.wait()


def on_device(n, n_fs, inputs, out_grad, pre_act, w_up, w_down_t):
    tok, d_model = inputs.shape
    group, cols = pre_act.shape
    shard = w_up.shape[0]
    chunks = max(1, shard // 256)
    factor = float(group * n) ** -0.5
    dma = pltpu.SemaphoreType.DMA
    vmem = pl.BlockSpec(memory_space=pltpu.VMEM)
    results = pl.pallas_call(
        functools.partial(kernel, n, n_fs, chunks, factor),
        out_shape=(
            pltpu.VMEM((tok, d_model), BF16),
            pltpu.VMEM((shard, cols), F32),
            pltpu.VMEM((shard, cols), F32),
        ),
        in_specs=[pl.BlockSpec(memory_space=pl.ANY)] * 5,
        out_specs=(vmem,) * 3,
        scratch_shapes=[
            pltpu.VMEM((2, group, d_model), BF16),
            pltpu.VMEM((2, n, shard, cols), BF16),
            pltpu.VMEM((2, group, cols), BF16),
            pltpu.VMEM((2, 2, n, shard, cols), BF16),
            pltpu.VMEM((n, 2, n_fs * tok, shard), BF16),
            pltpu.VMEM((n, n_fs * tok, shard), BF16),
            pltpu.VMEM((n, n_fs - 1, tok, shard), BF16),
            pltpu.VMEM((group, cols), BF16),
            dma((2,)),
            dma((2, chunks)),
            dma(()),
            dma(()),
        ],
        compiler_params=pltpu.CompilerParams(
            collective_id=0, has_side_effects=True, vmem_limit_bytes=56 * 2**20
        ),
    )(inputs, out_grad, pre_act, w_up, w_down_t)
    results = [pltpu.with_memory_space_constraint(a, pltpu.VMEM) for a in results]
    return pl.pallas_call(
        write_out,
        out_shape=[jax.ShapeDtypeStruct(a.shape, a.dtype) for a in results],
        in_specs=[vmem] * 3,
        out_specs=[pl.BlockSpec(memory_space=pl.ANY)] * 3,
        scratch_shapes=[dma((3,))],
        compiler_params=pltpu.CompilerParams(vmem_limit_bytes=2**20),
    )(*results)


def solution(mesh):
    rows = P(("rep", "fs", "tp"), None)
    blocks = P("rep", ("fs", "tp"))
    return jax.shard_map(
        functools.partial(on_device, mesh.shape["rep"], mesh.shape["fs"]),
        mesh=mesh,
        in_specs=(rows, rows, blocks, blocks, blocks),
        out_specs=(rows, blocks, blocks),
        check_vma=False,
    )
```

```python
import functools

import jax
import jax.numpy as jnp
from jax import lax
from jax.experimental import pallas as pl
from jax.experimental.pallas import tpu as pltpu
from jax.sharding import PartitionSpec as P

BF16 = jnp.bfloat16
F32 = jnp.float32


def kernel(
    n, n_fs, chunks, factor,
    x_ref, og_ref, pre_ref, wu_ref, wd_ref,
    gin_ref, gu_ref, gd_ref,
    rows_all, w_all, act, rs, tbuf, prec, frec, pre,
    zs, z_last, fsend, frecv,
):
    r, f, t = lax.axis_index("rep"), lax.axis_index("fs"), lax.axis_index("tp")
    tok, d_model = og_ref.shape
    shard, cols = wd_ref.shape
    crow = shard // chunks
    partner = {"tp": 1 - t}
    half = tok // 2
    own_tokens = pl.ds(pl.multiple_of((f * 2 + t) * tok, tok), tok)
    totals = (gd_ref, gu_ref)
    peer = [None, f + 1 - 2 * lax.rem(f, 2), lax.rem(f + 2, n_fs), n_fs - 1 - f]
    peers = [None] + [{"fs": peer[d]} for d in range(1, n_fs)]
    ahead = ({"rep": lax.rem(r + 1, n)}, {"rep": lax.rem(r + n - 1, n)})
    depth = (r, n - 1 - r)
    after = (n - 1 - r, r)
    has_next = (r < n - 1, r > 0)

    def remote(src, dst, send, recv, target):
        return pltpu.make_async_remote_copy(
            src_ref=src, dst_ref=dst, send_sem=send, recv_sem=recv,
            device_id=target, device_id_type=pl.DeviceIdType.MESH,
        )

    def rows_at(j):
        return pl.ds(pl.multiple_of(j * crow, crow), crow)

    def z_final(way, s, j):
        block = rs.at[1, way, s, rows_at(j), :]
        return remote(block, block, zs.at[way], z_last.at[way, j], ahead[way])

    def all_but_last_step(zr, xs, xr, cs, cr, ts, tr, ls, ready, answer):
        lead = crow + crow // 8 if chunks > 1 else crow // 2
        loads = [
            pltpu.make_async_copy(src, dst, ls.at[i])
            for i, (src, dst) in enumerate((
                (wd_ref.at[:lead], w_all.at[0, r, :lead]),
                (og_ref, rows_all.at[0, own_tokens, :]),
                (wu_ref, w_all.at[1, r]),
                (pre_ref, pre),
                (x_ref, rows_all.at[1, own_tokens, :]),
                (wd_ref.at[lead:], w_all.at[0, r, lead:]),
            ))
        ]
        barrier = pltpu.get_barrier_semaphore()
        @pl.when(has_next[0])
        def _():
            pl.semaphore_signal(barrier, inc=1, device_id=ahead[0])

        inner = (f > 0) & (f < n_fs - 1)

        @pl.when(jnp.logical_not(inner))
        def _():
            for d in (1, 2):
                pl.semaphore_signal(barrier, inc=1, device_id=peers[d])

        @pl.when(t == 0)
        def _():
            pl.semaphore_signal(barrier, inc=1, device_id=partner)

        for load in loads:
            load.start()
        greetings = jnp.where(r > 0, 1, 0) + jnp.where(inner, 2, 0) + t

        @pl.when(greetings > 0)
        def _():
            pl.semaphore_wait(barrier, greetings)

        @pl.when(has_next[1])
        def _():
            pl.semaphore_signal(answer, inc=1, device_id=ahead[1])

        @pl.when(inner)
        def _():
            for d in (1, 2):
                pl.semaphore_signal(ready, inc=1, device_id=peers[d])

        @pl.when(t == 1)
        def _():
            pl.semaphore_signal(ready, inc=1, device_id=partner)

        loads[0].wait()

        def rows_of(q, ff, tt):
            return rows_all.at[
                q, pl.ds(pl.multiple_of((ff * 2 + tt) * tok, tok), tok), :
            ]

        def z_copy(p, way, k, j, src, dst):
            return remote(src, dst, zs.at[way], zr.at[p, way, k, j], ahead[way])

        def send_own(p, way):
            for j in range(chunks):
                block = w_all.at[p, r, rows_at(j), :]
                z_copy(p, way, 0, j, block, block).start()

        def send_part(way, low, high):
            for j in range(chunks):
                a, b = max(low, j * crow), min(high, (j + 1) * crow)
                if a < b:
                    block = w_all.at[0, r, a:b, :]
                    z_copy(0, way, 0, j, block, block).start()

        def first_rows(q, count):
            return rows_all.at[q, pl.ds(0, count * tok), :]

        def half_rows(q, ff, side):
            at = (ff * 2 + t) * tok + side * half
            return rows_all.at[q, pl.ds(pl.multiple_of(at, half), half), :]

        def spread(q, block, d, stage):
            return remote(block, block, xs.at[q], xr.at[q, stage], peers[d])

        def swap(q, block):
            return remote(block, block, cs.at[q], cr.at[q], partner)

        def spread_start(q):
            own = rows_of(q, f, t)
            for d in (1, 2):
                spread(q, own, d, 0).start()
            swap(q, own).start()

        def spread_relay(q):
            spread(q, first_rows(q, 2), 1, 0).wait_recv()
            spread(q, half_rows(q, peer[2], 0), 1, 1).start()
            spread(q, half_rows(q, peer[1], 1), 2, 1).start()
            for d in (1, 2):
                swap(q, rows_of(q, peer[d], t)).start()

        def spread_pass(q):
            spread(q, first_rows(q, 1), 1, 1).wait_recv()
            swap(q, rows_of(q, peer[3], t)).start()

        def spread_end(q):
            swap(q, first_rows(q, n_fs)).wait_recv()

        def rest_of_first_sends():
            for way in range(2):
                @pl.when(has_next[way])
                def _(way=way):
                    send_part(way, lead, shard)

                @pl.when(depth[way] == 0)
                def _(way=way):
                    send_own(1, way)

        @pl.when(has_next[1])
        def _():
            send_part(1, 0, lead)

        @pl.when(has_next[0])
        def _():
            pl.semaphore_wait(answer, 1)
            send_part(0, 0, lead)

        loads[1].wait()

        @pl.when(jnp.logical_not(inner) | (t == 0))
        def _():
            pl.semaphore_wait(ready, jnp.where(inner, 0, 2) + 1 - t)

        spread_start(0)
        loads[2].wait()
        loads[5].wait()

        @pl.when(t == 0)
        def _():
            rest_of_first_sends()

        for load in loads[3:5]:
            load.wait()
        tile = 2 * tok

        def square(i, _):
            at = pl.ds(pl.multiple_of(i * tile, tile), tile)
            linear = jnp.maximum(pre[at, :].astype(F32), 0.0)
            act[0, at, :] = (linear * linear).astype(BF16)
            return 0

        lax.fori_loop(0, n_fs, square, 0)


        def partial(p, s, j):
            at = pl.ds(pl.multiple_of(s * shard + j * crow, crow), crow)
            return lax.dot_general(
                rows_all[p, :, at], act[p], (((0,), (0,)), ((), ())),
                preferred_element_type=F32,
            ) * factor

        def own_partial(p):
            def body(j, _):
                totals[p][rows_at(j), :] = partial(p, r, j)
                return 0

            lax.fori_loop(0, chunks, body, 0)

        def make_grad_pre(i, _):
            at = pl.ds(pl.multiple_of(i * tile, tile), tile)
            acc = jnp.zeros((tile, cols), F32)
            for s in range(n):
                acc += jnp.dot(
                    rows_all[0, at, s * shard:(s + 1) * shard], w_all[0, s],
                    preferred_element_type=F32,
                )
            linear = jnp.maximum(pre[at, :].astype(F32), 0.0)
            act[1, at, :] = (acc * 2.0 * linear).astype(BF16)
            return 0

        def cross(s):
            return remote(tbuf.at[s, 1 - t], prec.at[s], ts, tr.at[s], partner)

        def out_copy(s, d):
            rows = pl.ds(pl.multiple_of(peer[d] * tok, tok), tok)
            return remote(
                prec.at[s, rows, :], frec.at[s, d - 1],
                fsend, frecv, peers[d],
            )

        def block_term(s):
            def body(i, _):
                at = pl.ds(pl.multiple_of(i * tile, tile), tile)
                here = pl.ds(pl.multiple_of(i * tok, tok), tok)
                term = lax.dot_general(
                    act[1, at, :], w_all[1, s], (((1,), (1,)), ((), ())),
                    preferred_element_type=F32,
                ).astype(BF16)
                tbuf[s, 0, here, :] = term[:tok]
                tbuf[s, 1, here, :] = term[tok:]
                return 0

            lax.fori_loop(0, n_fs, body, 0)
            cross(s).start()

        def chip_sum(s):
            cross(s).wait_recv()

            def body(i, _):
                here = pl.ds(pl.multiple_of(i * tok, tok), tok)
                prec[s, here, :] = (
                    prec[s, here, :].astype(F32) + tbuf[s, t, here, :].astype(F32)
                ).astype(BF16)
                return 0

            lax.fori_loop(0, n_fs, body, 0)
            for d in range(1, n_fs):
                out_copy(s, d).start()

        def arrivals(step, way, j):
            d, h = depth[way], after[way]
            sign = 1 - 2 * way
            ag = step <= 2 * d
            p_ag = jnp.where(step > d, 1, 0)
            k = step - 1 - p_ag * d
            q = step - 2 * d - 1
            p_rs = jnp.where(q > h, 1, 0)
            i = q - p_rs * (h + 1) - jnp.where((d == 0) & (p_rs == 0), 1, 0)

            @pl.when(ag)
            def _():
                block = w_all.at[p_ag, r - sign * (1 + k), rows_at(j), :]
                z_copy(p_ag, way, k, j, block, block).wait_recv()

                @pl.when(h > 0)
                def _():
                    z_copy(p_ag, way, k + 1, j, block, block).start()

            @pl.when(jnp.logical_not(ag) & (i >= 0) & (i < h))
            def _():
                s = n - 1 - i if way == 0 else i
                term = partial(p_rs, s, j)
                block = rs.at[p_rs, way, s, rows_at(j), :]

                @pl.when(d > 0)
                def _():
                    z_copy(p_rs, way, d + i, j, block, block).wait_recv()
                    rs[p_rs, way, s, rows_at(j), :] = (
                        term + rs[p_rs, way, s, rows_at(j), :].astype(F32)
                    ).astype(BF16)

                @pl.when(d == 0)
                def _():
                    rs[p_rs, way, s, rows_at(j), :] = term.astype(BF16)

                final = (p_rs == 1) & (i == h - 1)

                @pl.when(final)
                def _():
                    z_final(way, s, j).start()

                @pl.when(jnp.logical_not(final))
                def _():
                    z_copy(p_rs, way, d + i + 1, j, block, block).start()

            @pl.when(jnp.logical_not(ag) & (i == h) & (d > 0))
            def _():
                block = rs.at[0, way, r, rows_at(j), :]
                z_copy(0, way, n - 1, j, block, block).wait_recv()
                gd_ref[rows_at(j), :] += rs[0, way, r, rows_at(j), :].astype(F32)

        def term_step(s):
            d = jnp.where(s < r, r, n - 1 - r)
            distance = jnp.where(s < r, r - s, s - r)
            return jnp.where(s == r, n - 1, jnp.maximum(d + distance, n - 1))

        def one_step(step, _):
            def body(j, _):
                for way in range(2):
                    arrivals(step, way, j)

                @pl.when((step <= 2) & (j == 0))
                def _():
                    spread_relay(step - 1)

                @pl.when((step == 1) & (j == 0) & (t == 1))
                def _():
                    rest_of_first_sends()
                return 0

            lax.fori_loop(0, chunks, body, 0)
            for way in range(2):
                @pl.when((depth[way] == step) & has_next[way])
                def _(way=way):
                    send_own(1, way)

            @pl.when(step == 1)
            def _():
                spread_start(1)
                spread_pass(0)
                spread_end(0)

            @pl.when(step == 2)
            def _():
                own_partial(0)

            @pl.when(step == n - 1)
            def _():
                spread_pass(1)
                lax.fori_loop(0, n_fs, make_grad_pre, 0)
                spread_end(1)

            @pl.when(step == n + 1)
            def _():
                own_partial(1)

            def terms(s, _):
                @pl.when(term_step(s) == step)
                def _():
                    block_term(s)

                @pl.when(term_step(s) + 1 == step)
                def _():
                    chip_sum(s)
                return 0

            lax.fori_loop(0, n, terms, 0)
            return 0

        lax.fori_loop(1, 2 * n, one_step, 0)
        remote(prec, prec, ts, tr.at[0], partner).wait_send()
        for q in range(2):
            spread(q, first_rows(q, n_fs - 1), 1, 0).wait_send()
            swap(q, first_rows(q, n_fs)).wait_send()

    dma = pltpu.SemaphoreType.DMA
    pl.run_scoped(
        all_but_last_step,
        dma((2, 2, n, chunks)), dma((2,)), dma((2, 2)), dma((2,)), dma((2,)),
        dma(()), dma((n,)), dma((6,)), pltpu.SemaphoreType.REGULAR,
        pltpu.SemaphoreType.REGULAR,
    )

    def last(j, _):
        for way in range(2):
            @pl.when(depth[way] > 0)
            def _(way=way):
                z_final(way, r, j).wait_recv()
                gu_ref[rows_at(j), :] += rs[1, way, r, rows_at(j), :].astype(F32)
        return 0

    lax.fori_loop(0, chunks - 1, last, 0)
    own_rows = pl.ds(pl.multiple_of(f * tok, tok), tok)
    remote(frec, frec, fsend, frecv, peers[1]).wait()
    for s in range(n):
        acc = prec[s, own_rows, :].astype(F32)
        for d in range(1, n_fs):
            acc += frec[s, d - 1].astype(F32)
        gin_ref[:, s * shard:(s + 1) * shard] = acc.astype(BF16)
    for way in range(2):
        @pl.when(has_next[way])
        def _(way=way):
            remote(w_all, w_all, zs.at[way], z_last.at[way, 0], ahead[way]).wait_send()
    lax.fori_loop(chunks - 1, chunks, last, 0)


def write_out(*refs):
    copies = [
        pltpu.make_async_copy(refs[i], refs[3 + i], refs[6].at[i]) for i in range(3)
    ]
    for copy in copies:
        copy.start()
    for copy in copies:
        copy.wait()


def on_device(n, n_fs, inputs, out_grad, pre_act, w_up, w_down_t):
    tok, d_model = inputs.shape
    group, cols = pre_act.shape
    shard = w_up.shape[0]
    chunks = max(1, shard // 256)
    factor = float(group * n) ** -0.5
    dma = pltpu.SemaphoreType.DMA
    vmem = pl.BlockSpec(memory_space=pltpu.VMEM)
    results = pl.pallas_call(
        functools.partial(kernel, n, n_fs, chunks, factor),
        out_shape=(
            pltpu.VMEM((tok, d_model), BF16),
            pltpu.VMEM((shard, cols), F32),
            pltpu.VMEM((shard, cols), F32),
        ),
        in_specs=[pl.BlockSpec(memory_space=pl.ANY)] * 5,
        out_specs=(vmem,) * 3,
        scratch_shapes=[
            pltpu.VMEM((2, group, d_model), BF16),
            pltpu.VMEM((2, n, shard, cols), BF16),
            pltpu.VMEM((2, group, cols), BF16),
            pltpu.VMEM((2, 2, n, shard, cols), BF16),
            pltpu.VMEM((n, 2, n_fs * tok, shard), BF16),
            pltpu.VMEM((n, n_fs * tok, shard), BF16),
            pltpu.VMEM((n, n_fs - 1, tok, shard), BF16),
            pltpu.VMEM((group, cols), BF16),
            dma((2,)),
            dma((2, chunks)),
            dma(()),
            dma(()),
        ],
        compiler_params=pltpu.CompilerParams(
            collective_id=0, has_side_effects=True, vmem_limit_bytes=56 * 2**20
        ),
    )(inputs, out_grad, pre_act, w_up, w_down_t)
    results = [pltpu.with_memory_space_constraint(a, pltpu.VMEM) for a in results]
    return pl.pallas_call(
        write_out,
        out_shape=[jax.ShapeDtypeStruct(a.shape, a.dtype) for a in results],
        in_specs=[vmem] * 3,
        out_specs=[pl.BlockSpec(memory_space=pl.ANY)] * 3,
        scratch_shapes=[dma((3,))],
        compiler_params=pltpu.CompilerParams(vmem_limit_bytes=2**20),
    )(*results)


def solution(mesh):
    rows = P(("rep", "fs", "tp"), None)
    blocks = P("rep", ("fs", "tp"))
    return jax.shard_map(
        functools.partial(on_device, mesh.shape["rep"], mesh.shape["fs"]),
        mesh=mesh,
        in_specs=(rows, rows, blocks, blocks, blocks),
        out_specs=(rows, blocks, blocks),
        check_vma=False,
    )
```

```python
import functools

import jax
import jax.numpy as jnp
from jax import lax
from jax.experimental import pallas as pl
from jax.experimental.pallas import tpu as pltpu
from jax.sharding import PartitionSpec as P

BF16 = jnp.bfloat16
F32 = jnp.float32


def kernel(
    n, n_fs, chunks, factor,
    x_ref, og_ref, pre_ref, wu_ref, wd_ref,
    gin_ref, gu_ref, gd_ref,
    rows_all, w_all, act, rs, tbuf, prec, frec, pre,
    zs, z_last, fsend, frecv,
):
    r, f, t = lax.axis_index("rep"), lax.axis_index("fs"), lax.axis_index("tp")
    tok, d_model = og_ref.shape
    shard, cols = wd_ref.shape
    crow = shard // chunks
    partner = {"tp": 1 - t}
    half = tok // 2
    own_tokens = pl.ds(pl.multiple_of((f * 2 + t) * tok, tok), tok)
    totals = (gd_ref, gu_ref)
    peer = [None, f + 1 - 2 * lax.rem(f, 2), lax.rem(f + 2, n_fs), n_fs - 1 - f]
    peers = [None] + [{"fs": peer[d]} for d in range(1, n_fs)]
    ahead = ({"rep": lax.rem(r + 1, n)}, {"rep": lax.rem(r + n - 1, n)})
    depth = (r, n - 1 - r)
    after = (n - 1 - r, r)
    has_next = (r < n - 1, r > 0)

    def remote(src, dst, send, recv, target):
        return pltpu.make_async_remote_copy(
            src_ref=src, dst_ref=dst, send_sem=send, recv_sem=recv,
            device_id=target, device_id_type=pl.DeviceIdType.MESH,
        )

    def rows_at(j):
        return pl.ds(pl.multiple_of(j * crow, crow), crow)

    def z_final(way, s, j):
        block = rs.at[1, way, s, rows_at(j), :]
        return remote(block, block, zs.at[way], z_last.at[way, j], ahead[way])

    def all_but_last_step(zr, xs, xr, cs, cr, ts, tr, ls, ready, answer):
        lead = crow + crow // 8 if chunks > 1 else crow // 2
        loads = [
            pltpu.make_async_copy(src, dst, ls.at[i])
            for i, (src, dst) in enumerate((
                (wd_ref.at[:lead], w_all.at[0, r, :lead]),
                (og_ref, rows_all.at[0, own_tokens, :]),
                (wu_ref, w_all.at[1, r]),
                (pre_ref, pre),
                (x_ref, rows_all.at[1, own_tokens, :]),
                (wd_ref.at[lead:], w_all.at[0, r, lead:]),
            ))
        ]
        barrier = pltpu.get_barrier_semaphore()
        @pl.when(has_next[0])
        def _():
            pl.semaphore_signal(barrier, inc=1, device_id=ahead[0])

        inner = (f > 0) & (f < n_fs - 1)

        @pl.when(jnp.logical_not(inner))
        def _():
            for d in (1, 2):
                pl.semaphore_signal(barrier, inc=1, device_id=peers[d])

        @pl.when(t == 0)
        def _():
            pl.semaphore_signal(barrier, inc=1, device_id=partner)

        for load in loads:
            load.start()
        greetings = jnp.where(r > 0, 1, 0) + jnp.where(inner, 2, 0) + t

        @pl.when(greetings > 0)
        def _():
            pl.semaphore_wait(barrier, greetings)

        @pl.when(has_next[1])
        def _():
            pl.semaphore_signal(answer, inc=1, device_id=ahead[1])

        @pl.when(inner)
        def _():
            for d in (1, 2):
                pl.semaphore_signal(ready, inc=1, device_id=peers[d])

        @pl.when(t == 1)
        def _():
            pl.semaphore_signal(ready, inc=1, device_id=partner)

        loads[0].wait()

        def rows_of(q, ff, tt):
            return rows_all.at[
                q, pl.ds(pl.multiple_of((ff * 2 + tt) * tok, tok), tok), :
            ]

        def z_copy(p, way, k, j, src, dst):
            return remote(src, dst, zs.at[way], zr.at[p, way, k, j], ahead[way])

        def send_own(p, way):
            for j in range(chunks):
                block = w_all.at[p, r, rows_at(j), :]
                z_copy(p, way, 0, j, block, block).start()

        def send_part(way, low, high):
            for j in range(chunks):
                a, b = max(low, j * crow), min(high, (j + 1) * crow)
                if a < b:
                    block = w_all.at[0, r, a:b, :]
                    z_copy(0, way, 0, j, block, block).start()

        def first_rows(q, count):
            return rows_all.at[q, pl.ds(0, count * tok), :]

        def half_rows(q, ff, side):
            at = (ff * 2 + t) * tok + side * half
            return rows_all.at[q, pl.ds(pl.multiple_of(at, half), half), :]

        def spread(q, block, d, stage):
            return remote(block, block, xs.at[q], xr.at[q, stage], peers[d])

        def swap(q, block):
            return remote(block, block, cs.at[q], cr.at[q], partner)

        def spread_start(q):
            own = rows_of(q, f, t)
            for d in (1, 2):
                spread(q, own, d, 0).start()
            swap(q, own).start()

        def spread_relay(q):
            spread(q, first_rows(q, 2), 1, 0).wait_recv()
            spread(q, half_rows(q, peer[2], 0), 1, 1).start()
            spread(q, half_rows(q, peer[1], 1), 2, 1).start()
            for d in (1, 2):
                swap(q, rows_of(q, peer[d], t)).start()

        def spread_pass(q):
            spread(q, first_rows(q, 1), 1, 1).wait_recv()
            swap(q, rows_of(q, peer[3], t)).start()

        def spread_end(q):
            swap(q, first_rows(q, n_fs)).wait_recv()

        def rest_of_first_sends():
            for way in range(2):
                @pl.when(has_next[way])
                def _(way=way):
                    send_part(way, lead, shard)

                @pl.when(depth[way] == 0)
                def _(way=way):
                    send_own(1, way)

        @pl.when(has_next[1])
        def _():
            send_part(1, 0, lead)

        @pl.when(has_next[0])
        def _():
            pl.semaphore_wait(answer, 1)
            send_part(0, 0, lead)

        loads[1].wait()

        @pl.when(jnp.logical_not(inner) | (t == 0))
        def _():
            pl.semaphore_wait(ready, jnp.where(inner, 0, 2) + 1 - t)

        spread_start(0)
        loads[2].wait()
        loads[5].wait()

        @pl.when(t == 0)
        def _():
            rest_of_first_sends()

        for load in loads[3:5]:
            load.wait()
        tile = 2 * tok

        def square(i, _):
            at = pl.ds(pl.multiple_of(i * tile, tile), tile)
            linear = jnp.maximum(pre[at, :].astype(F32), 0.0)
            act[0, at, :] = (linear * linear).astype(BF16)
            return 0

        lax.fori_loop(0, n_fs, square, 0)


        def partial(p, s, j):
            at = pl.ds(pl.multiple_of(s * shard + j * crow, crow), crow)
            return lax.dot_general(
                rows_all[p, :, at], act[p], (((0,), (0,)), ((), ())),
                preferred_element_type=F32,
            ) * factor

        def own_partial(p):
            def body(j, _):
                totals[p][rows_at(j), :] = partial(p, r, j)
                return 0

            lax.fori_loop(0, chunks, body, 0)

        def make_grad_pre(i, _):
            at = pl.ds(pl.multiple_of(i * tile, tile), tile)
            acc = jnp.zeros((tile, cols), F32)
            for s in range(n):
                acc += jnp.dot(
                    rows_all[0, at, s * shard:(s + 1) * shard], w_all[0, s],
                    preferred_element_type=F32,
                )
            linear = jnp.maximum(pre[at, :].astype(F32), 0.0)
            act[1, at, :] = (acc * 2.0 * linear).astype(BF16)
            return 0

        def cross(s):
            return remote(tbuf.at[s, 1 - t], prec.at[s], ts, tr.at[s], partner)

        def out_copy(s, d):
            rows = pl.ds(pl.multiple_of(peer[d] * tok, tok), tok)
            return remote(
                prec.at[s, rows, :], frec.at[s, d - 1],
                fsend, frecv, peers[d],
            )

        def block_term(s):
            def body(i, _):
                at = pl.ds(pl.multiple_of(i * tile, tile), tile)
                here = pl.ds(pl.multiple_of(i * tok, tok), tok)
                term = lax.dot_general(
                    act[1, at, :], w_all[1, s], (((1,), (1,)), ((), ())),
                    preferred_element_type=F32,
                ).astype(BF16)
                tbuf[s, 0, here, :] = term[:tok]
                tbuf[s, 1, here, :] = term[tok:]
                return 0

            lax.fori_loop(0, n_fs, body, 0)
            cross(s).start()

        def chip_sum(s):
            cross(s).wait_recv()

            def body(i, _):
                here = pl.ds(pl.multiple_of(i * tok, tok), tok)
                prec[s, here, :] = (
                    prec[s, here, :].astype(F32) + tbuf[s, t, here, :].astype(F32)
                ).astype(BF16)
                return 0

            lax.fori_loop(0, n_fs, body, 0)
            for d in range(1, n_fs):
                out_copy(s, d).start()

        def arrivals(step, way, j):
            d, h = depth[way], after[way]
            sign = 1 - 2 * way
            ag = step <= 2 * d
            p_ag = jnp.where(step > d, 1, 0)
            k = step - 1 - p_ag * d
            q = step - 2 * d - 1
            p_rs = jnp.where(q > h, 1, 0)
            i = q - p_rs * (h + 1) - jnp.where((d == 0) & (p_rs == 0), 1, 0)

            @pl.when(ag)
            def _():
                block = w_all.at[p_ag, r - sign * (1 + k), rows_at(j), :]
                z_copy(p_ag, way, k, j, block, block).wait_recv()

                @pl.when(h > 0)
                def _():
                    z_copy(p_ag, way, k + 1, j, block, block).start()

            @pl.when(jnp.logical_not(ag) & (i >= 0) & (i < h))
            def _():
                s = n - 1 - i if way == 0 else i
                term = partial(p_rs, s, j)
                block = rs.at[p_rs, way, s, rows_at(j), :]

                @pl.when(d > 0)
                def _():
                    z_copy(p_rs, way, d + i, j, block, block).wait_recv()
                    rs[p_rs, way, s, rows_at(j), :] = (
                        term + rs[p_rs, way, s, rows_at(j), :].astype(F32)
                    ).astype(BF16)

                @pl.when(d == 0)
                def _():
                    rs[p_rs, way, s, rows_at(j), :] = term.astype(BF16)

                final = (p_rs == 1) & (i == h - 1)

                @pl.when(final)
                def _():
                    z_final(way, s, j).start()

                @pl.when(jnp.logical_not(final))
                def _():
                    z_copy(p_rs, way, d + i + 1, j, block, block).start()

            @pl.when(jnp.logical_not(ag) & (i == h) & (d > 0))
            def _():
                block = rs.at[0, way, r, rows_at(j), :]
                z_copy(0, way, n - 1, j, block, block).wait_recv()
                gd_ref[rows_at(j), :] += rs[0, way, r, rows_at(j), :].astype(F32)

        def term_step(s):
            d = jnp.where(s < r, r, n - 1 - r)
            distance = jnp.where(s < r, r - s, s - r)
            return jnp.where(s == r, n - 1, jnp.maximum(d + distance, n - 1))

        def one_step(step, _):
            def body(j, _):
                for way in range(2):
                    arrivals(step, way, j)

                @pl.when((step <= 2) & (j == 0))
                def _():
                    spread_relay(step - 1)

                @pl.when((step == 1) & (j == 0) & (t == 1))
                def _():
                    rest_of_first_sends()
                return 0

            lax.fori_loop(0, chunks, body, 0)
            for way in range(2):
                @pl.when((depth[way] == step) & has_next[way])
                def _(way=way):
                    send_own(1, way)

            @pl.when(step == 1)
            def _():
                spread_start(1)
                spread_pass(0)
                spread_end(0)

            @pl.when(step == 2)
            def _():
                own_partial(0)

            @pl.when(step == n - 1)
            def _():
                spread_pass(1)
                lax.fori_loop(0, n_fs, make_grad_pre, 0)
                spread_end(1)

            @pl.when(step == n + 1)
            def _():
                own_partial(1)

            def terms(s, _):
                @pl.when(term_step(s) == step)
                def _():
                    block_term(s)

                @pl.when(term_step(s) + 1 == step)
                def _():
                    chip_sum(s)
                return 0

            lax.fori_loop(0, n, terms, 0)
            return 0

        lax.fori_loop(1, 2 * n, one_step, 0)
        remote(prec, prec, ts, tr.at[0], partner).wait_send()
        for q in range(2):
            spread(q, first_rows(q, n_fs - 1), 1, 0).wait_send()
            swap(q, first_rows(q, n_fs)).wait_send()

    dma = pltpu.SemaphoreType.DMA
    pl.run_scoped(
        all_but_last_step,
        dma((2, 2, n, chunks)), dma((2,)), dma((2, 2)), dma((2,)), dma((2,)),
        dma(()), dma((n,)), dma((6,)), pltpu.SemaphoreType.REGULAR,
        pltpu.SemaphoreType.REGULAR,
    )

    def last(j, _):
        for way in range(2):
            @pl.when(depth[way] > 0)
            def _(way=way):
                z_final(way, r, j).wait_recv()

        @pl.when((depth[0] > 0) & (depth[1] > 0))
        def _():
            gu_ref[rows_at(j), :] += (
                rs[1, 0, r, rows_at(j), :].astype(F32)
                + rs[1, 1, r, rows_at(j), :].astype(F32)
            )

        for way in range(2):
            @pl.when((depth[way] > 0) & (depth[1 - way] == 0))
            def _(way=way):
                gu_ref[rows_at(j), :] += rs[1, way, r, rows_at(j), :].astype(F32)
        return 0

    lax.fori_loop(0, chunks - 1, last, 0)
    own_rows = pl.ds(pl.multiple_of(f * tok, tok), tok)
    remote(frec, frec, fsend, frecv, peers[1]).wait()
    for s in range(n):
        acc = prec[s, own_rows, :].astype(F32)
        for d in range(1, n_fs):
            acc += frec[s, d - 1].astype(F32)
        gin_ref[:, s * shard:(s + 1) * shard] = acc.astype(BF16)
    for way in range(2):
        @pl.when(has_next[way])
        def _(way=way):
            remote(w_all, w_all, zs.at[way], z_last.at[way, 0], ahead[way]).wait_send()
    lax.fori_loop(chunks - 1, chunks, last, 0)


def write_out(*refs):
    copies = [
        pltpu.make_async_copy(refs[i], refs[3 + i], refs[6].at[i]) for i in range(3)
    ]
    for i, copy in ((2, copies[2]), (1, copies[1]), (0, copies[0])):
        copy.start(priority=i % 2)
    for copy in copies:
        copy.wait()


def on_device(n, n_fs, inputs, out_grad, pre_act, w_up, w_down_t):
    tok, d_model = inputs.shape
    group, cols = pre_act.shape
    shard = w_up.shape[0]
    chunks = max(1, shard // 256)
    factor = float(group * n) ** -0.5
    dma = pltpu.SemaphoreType.DMA
    vmem = pl.BlockSpec(memory_space=pltpu.VMEM)
    results = pl.pallas_call(
        functools.partial(kernel, n, n_fs, chunks, factor),
        out_shape=(
            pltpu.VMEM((tok, d_model), BF16),
            pltpu.VMEM((shard, cols), F32),
            pltpu.VMEM((shard, cols), F32),
        ),
        in_specs=[pl.BlockSpec(memory_space=pl.ANY)] * 5,
        out_specs=(vmem,) * 3,
        scratch_shapes=[
            pltpu.VMEM((2, group, d_model), BF16),
            pltpu.VMEM((2, n, shard, cols), BF16),
            pltpu.VMEM((2, group, cols), BF16),
            pltpu.VMEM((2, 2, n, shard, cols), BF16),
            pltpu.VMEM((n, 2, n_fs * tok, shard), BF16),
            pltpu.VMEM((n, n_fs * tok, shard), BF16),
            pltpu.VMEM((n, n_fs - 1, tok, shard), BF16),
            pltpu.VMEM((group, cols), BF16),
            dma((2,)),
            dma((2, chunks)),
            dma(()),
            dma(()),
        ],
        compiler_params=pltpu.CompilerParams(
            collective_id=0, has_side_effects=True, vmem_limit_bytes=56 * 2**20
        ),
    )(inputs, out_grad, pre_act, w_up, w_down_t)
    results = [pltpu.with_memory_space_constraint(a, pltpu.VMEM) for a in results]
    return pl.pallas_call(
        write_out,
        out_shape=[jax.ShapeDtypeStruct(a.shape, a.dtype) for a in results],
        in_specs=[vmem] * 3,
        out_specs=[pl.BlockSpec(memory_space=pl.ANY)] * 3,
        scratch_shapes=[dma((3,))],
        compiler_params=pltpu.CompilerParams(vmem_limit_bytes=2**20),
    )(*results)


def solution(mesh):
    rows = P(("rep", "fs", "tp"), None)
    blocks = P("rep", ("fs", "tp"))
    return jax.shard_map(
        functools.partial(on_device, mesh.shape["rep"], mesh.shape["fs"]),
        mesh=mesh,
        in_specs=(rows, rows, blocks, blocks, blocks),
        out_specs=(rows, blocks, blocks),
        check_vma=False,
    )
```

```python
import functools

import jax
import jax.numpy as jnp
from jax import lax
from jax.experimental import pallas as pl
from jax.experimental.pallas import tpu as pltpu
from jax.sharding import PartitionSpec as P

BF16 = jnp.bfloat16
F32 = jnp.float32


def kernel(
    n, n_fs, chunks, factor,
    x_ref, og_ref, pre_ref, wu_ref, wd_ref,
    gin_ref, gu_ref, gd_ref,
    rows_all, w_all, act, rs, tbuf, prec, frec, pre,
    zs, z_last, fsend, frecv,
):
    r, f, t = lax.axis_index("rep"), lax.axis_index("fs"), lax.axis_index("tp")
    tok, d_model = og_ref.shape
    shard, cols = wd_ref.shape
    crow = shard // chunks
    partner = {"tp": 1 - t}
    half = tok // 2
    own_tokens = pl.ds(pl.multiple_of((f * 2 + t) * tok, tok), tok)
    totals = (gd_ref, gu_ref)
    peer = [None, f + 1 - 2 * lax.rem(f, 2), lax.rem(f + 2, n_fs), n_fs - 1 - f]
    peers = [None] + [{"fs": peer[d]} for d in range(1, n_fs)]
    ahead = ({"rep": lax.rem(r + 1, n)}, {"rep": lax.rem(r + n - 1, n)})
    depth = (r, n - 1 - r)
    after = (n - 1 - r, r)
    has_next = (r < n - 1, r > 0)

    def remote(src, dst, send, recv, target):
        return pltpu.make_async_remote_copy(
            src_ref=src, dst_ref=dst, send_sem=send, recv_sem=recv,
            device_id=target, device_id_type=pl.DeviceIdType.MESH,
        )

    def rows_at(j):
        return pl.ds(pl.multiple_of(j * crow, crow), crow)

    def z_final(way, s, j):
        block = rs.at[1, way, s, rows_at(j), :]
        return remote(block, block, zs.at[way], z_last.at[way, j], ahead[way])

    def all_but_last_step(zr, xs, xr, cs, cr, ts, tr, ls, ready, answer):
        lead = crow + crow // 8 if chunks > 1 else crow // 2
        loads = [
            pltpu.make_async_copy(src, dst, ls.at[i])
            for i, (src, dst) in enumerate((
                (wd_ref.at[:lead], w_all.at[0, r, :lead]),
                (og_ref, rows_all.at[0, own_tokens, :]),
                (wu_ref, w_all.at[1, r]),
                (pre_ref, pre),
                (x_ref, rows_all.at[1, own_tokens, :]),
                (wd_ref.at[lead:], w_all.at[0, r, lead:]),
            ))
        ]
        barrier = pltpu.get_barrier_semaphore()
        @pl.when(has_next[0])
        def _():
            pl.semaphore_signal(barrier, inc=1, device_id=ahead[0])

        inner = (f > 0) & (f < n_fs - 1)

        @pl.when(jnp.logical_not(inner))
        def _():
            for d in (1, 2):
                pl.semaphore_signal(barrier, inc=1, device_id=peers[d])

        @pl.when(t == 0)
        def _():
            pl.semaphore_signal(barrier, inc=1, device_id=partner)

        for load in loads:
            load.start()
        greetings = jnp.where(r > 0, 1, 0) + jnp.where(inner, 2, 0) + t

        @pl.when(greetings > 0)
        def _():
            pl.semaphore_wait(barrier, greetings)

        @pl.when(has_next[1])
        def _():
            pl.semaphore_signal(answer, inc=1, device_id=ahead[1])

        @pl.when(inner)
        def _():
            for d in (1, 2):
                pl.semaphore_signal(ready, inc=1, device_id=peers[d])

        @pl.when(t == 1)
        def _():
            pl.semaphore_signal(ready, inc=1, device_id=partner)

        loads[0].wait()

        def rows_of(q, ff, tt):
            return rows_all.at[
                q, pl.ds(pl.multiple_of((ff * 2 + tt) * tok, tok), tok), :
            ]

        def z_copy(p, way, k, j, src, dst):
            return remote(src, dst, zs.at[way], zr.at[p, way, k, j], ahead[way])

        def send_own(p, way):
            for j in range(chunks):
                block = w_all.at[p, r, rows_at(j), :]
                z_copy(p, way, 0, j, block, block).start()

        def send_part(way, low, high):
            for j in range(chunks):
                a, b = max(low, j * crow), min(high, (j + 1) * crow)
                if a < b:
                    block = w_all.at[0, r, a:b, :]
                    z_copy(0, way, 0, j, block, block).start()

        def first_rows(q, count):
            return rows_all.at[q, pl.ds(0, count * tok), :]

        def half_rows(q, ff, side):
            at = (ff * 2 + t) * tok + side * half
            return rows_all.at[q, pl.ds(pl.multiple_of(at, half), half), :]

        def spread(q, block, d, stage):
            return remote(block, block, xs.at[q], xr.at[q, stage], peers[d])

        def swap(q, block):
            return remote(block, block, cs.at[q], cr.at[q], partner)

        def spread_start(q):
            own = rows_of(q, f, t)
            for d in (1, 2):
                spread(q, own, d, 0).start()
            swap(q, own).start()

        def spread_relay(q):
            spread(q, first_rows(q, 2), 1, 0).wait_recv()
            spread(q, half_rows(q, peer[2], 0), 1, 1).start()
            spread(q, half_rows(q, peer[1], 1), 2, 1).start()
            for d in (1, 2):
                swap(q, rows_of(q, peer[d], t)).start()

        def spread_pass(q):
            spread(q, first_rows(q, 1), 1, 1).wait_recv()
            swap(q, rows_of(q, peer[3], t)).start()

        def spread_end(q):
            swap(q, first_rows(q, n_fs)).wait_recv()

        def rest_of_first_sends():
            for way in range(2):
                @pl.when(has_next[way])
                def _(way=way):
                    send_part(way, lead, shard)

                @pl.when(depth[way] == 0)
                def _(way=way):
                    send_own(1, way)

        @pl.when(has_next[1])
        def _():
            send_part(1, 0, lead)

        @pl.when(has_next[0])
        def _():
            pl.semaphore_wait(answer, 1)
            send_part(0, 0, lead)

        loads[1].wait()

        @pl.when(jnp.logical_not(inner) | (t == 0))
        def _():
            pl.semaphore_wait(ready, jnp.where(inner, 0, 2) + 1 - t)

        spread_start(0)
        loads[2].wait()
        loads[5].wait()

        @pl.when(t == 0)
        def _():
            rest_of_first_sends()

        for load in loads[3:5]:
            load.wait()
        tile = 2 * tok

        def square(i, _):
            at = pl.ds(pl.multiple_of(i * tile, tile), tile)
            linear = jnp.maximum(pre[at, :].astype(F32), 0.0)
            act[0, at, :] = (linear * linear).astype(BF16)
            return 0

        lax.fori_loop(0, n_fs, square, 0)


        def partial(p, s, j):
            at = pl.ds(pl.multiple_of(s * shard + j * crow, crow), crow)
            return lax.dot_general(
                rows_all[p, :, at], act[p], (((0,), (0,)), ((), ())),
                preferred_element_type=F32,
            ) * factor

        def own_partial(p):
            def body(j, _):
                totals[p][rows_at(j), :] = partial(p, r, j)
                return 0

            lax.fori_loop(0, chunks, body, 0)

        def make_grad_pre(i, _):
            at = pl.ds(pl.multiple_of(i * tile, tile), tile)
            acc = jnp.zeros((tile, cols), F32)
            for s in range(n):
                acc += jnp.dot(
                    rows_all[0, at, s * shard:(s + 1) * shard], w_all[0, s],
                    preferred_element_type=F32,
                )
            linear = jnp.maximum(pre[at, :].astype(F32), 0.0)
            act[1, at, :] = (acc * 2.0 * linear).astype(BF16)
            return 0

        def cross(s):
            return remote(tbuf.at[s, 1 - t], prec.at[s], ts, tr.at[s], partner)

        def out_copy(s, d):
            rows = pl.ds(pl.multiple_of(peer[d] * tok, tok), tok)
            return remote(
                prec.at[s, rows, :], frec.at[s, d - 1],
                fsend, frecv, peers[d],
            )

        def block_term(s):
            def body(i, _):
                at = pl.ds(pl.multiple_of(i * tile, tile), tile)
                here = pl.ds(pl.multiple_of(i * tok, tok), tok)
                term = lax.dot_general(
                    act[1, at, :], w_all[1, s], (((1,), (1,)), ((), ())),
                    preferred_element_type=F32,
                ).astype(BF16)
                tbuf[s, 0, here, :] = term[:tok]
                tbuf[s, 1, here, :] = term[tok:]
                return 0

            lax.fori_loop(0, n_fs, body, 0)
            cross(s).start()

        def chip_sum(s):
            cross(s).wait_recv()

            def body(i, _):
                here = pl.ds(pl.multiple_of(i * tok, tok), tok)
                prec[s, here, :] = (
                    prec[s, here, :].astype(F32) + tbuf[s, t, here, :].astype(F32)
                ).astype(BF16)
                return 0

            lax.fori_loop(0, n_fs, body, 0)
            for d in range(1, n_fs):
                out_copy(s, d).start()

        def arrivals(step, way, j):
            d, h = depth[way], after[way]
            sign = 1 - 2 * way
            ag = step <= 2 * d
            p_ag = jnp.where(step > d, 1, 0)
            k = step - 1 - p_ag * d
            q = step - 2 * d - 1
            p_rs = jnp.where(q > h, 1, 0)
            i = q - p_rs * (h + 1) - jnp.where((d == 0) & (p_rs == 0), 1, 0)

            @pl.when(ag)
            def _():
                block = w_all.at[p_ag, r - sign * (1 + k), rows_at(j), :]
                z_copy(p_ag, way, k, j, block, block).wait_recv()

                @pl.when(h > 0)
                def _():
                    z_copy(p_ag, way, k + 1, j, block, block).start()

            @pl.when(jnp.logical_not(ag) & (i >= 0) & (i < h))
            def _():
                s = n - 1 - i if way == 0 else i
                term = partial(p_rs, s, j)
                block = rs.at[p_rs, way, s, rows_at(j), :]

                @pl.when(d > 0)
                def _():
                    z_copy(p_rs, way, d + i, j, block, block).wait_recv()
                    rs[p_rs, way, s, rows_at(j), :] = (
                        term + rs[p_rs, way, s, rows_at(j), :].astype(F32)
                    ).astype(BF16)

                @pl.when(d == 0)
                def _():
                    rs[p_rs, way, s, rows_at(j), :] = term.astype(BF16)

                final = (p_rs == 1) & (i == h - 1)

                @pl.when(final)
                def _():
                    z_final(way, s, j).start()

                @pl.when(jnp.logical_not(final))
                def _():
                    z_copy(p_rs, way, d + i + 1, j, block, block).start()

            @pl.when(jnp.logical_not(ag) & (i == h) & (d > 0))
            def _():
                block = rs.at[0, way, r, rows_at(j), :]
                z_copy(0, way, n - 1, j, block, block).wait_recv()
                gd_ref[rows_at(j), :] += rs[0, way, r, rows_at(j), :].astype(F32)

        def term_step(s):
            d = jnp.where(s < r, r, n - 1 - r)
            distance = jnp.where(s < r, r - s, s - r)
            return jnp.where(s == r, n - 1, jnp.maximum(d + distance, n - 1))

        def one_step(step, _):
            def body(j, _):
                for way in range(2):
                    arrivals(step, way, j)

                @pl.when((step <= 2) & (j == 0))
                def _():
                    spread_relay(step - 1)

                @pl.when((step == 1) & (j == 0) & (t == 1))
                def _():
                    rest_of_first_sends()
                return 0

            lax.fori_loop(0, chunks, body, 0)
            for way in range(2):
                @pl.when((depth[way] == step) & has_next[way])
                def _(way=way):
                    send_own(1, way)

            @pl.when(step == 1)
            def _():
                spread_start(1)
                spread_pass(0)
                spread_end(0)

            @pl.when(step == 2)
            def _():
                own_partial(0)

            @pl.when(step == n - 1)
            def _():
                spread_pass(1)
                lax.fori_loop(0, n_fs, make_grad_pre, 0)
                spread_end(1)

            @pl.when(step == n + 1)
            def _():
                own_partial(1)

            def terms(s, _):
                @pl.when(term_step(s) == step)
                def _():
                    block_term(s)

                @pl.when(term_step(s) + 1 == step)
                def _():
                    chip_sum(s)
                return 0

            lax.fori_loop(0, n, terms, 0)
            return 0

        lax.fori_loop(1, 2 * n, one_step, 0)
        remote(prec, prec, ts, tr.at[0], partner).wait_send()
        for q in range(2):
            spread(q, first_rows(q, n_fs - 1), 1, 0).wait_send()
            swap(q, first_rows(q, n_fs)).wait_send()

    dma = pltpu.SemaphoreType.DMA
    pl.run_scoped(
        all_but_last_step,
        dma((2, 2, n, chunks)), dma((2,)), dma((2, 2)), dma((2,)), dma((2,)),
        dma(()), dma((n,)), dma((6,)), pltpu.SemaphoreType.REGULAR,
        pltpu.SemaphoreType.REGULAR,
    )

    def last(j, _):
        for way in range(2):
            @pl.when(depth[way] > 0)
            def _(way=way):
                z_final(way, r, j).wait_recv()
                gu_ref[rows_at(j), :] += rs[1, way, r, rows_at(j), :].astype(F32)
        return 0

    lax.fori_loop(0, chunks - 1, last, 0)
    own_rows = pl.ds(pl.multiple_of(f * tok, tok), tok)
    remote(frec, frec, fsend, frecv, peers[1]).wait()
    for s in range(n):
        acc = prec[s, own_rows, :].astype(F32)
        for d in range(1, n_fs):
            acc += frec[s, d - 1].astype(F32)
        gin_ref[:, s * shard:(s + 1) * shard] = acc.astype(BF16)
    for way in range(2):
        @pl.when(has_next[way])
        def _(way=way):
            remote(w_all, w_all, zs.at[way], z_last.at[way, 0], ahead[way]).wait_send()
    lax.fori_loop(chunks - 1, chunks, last, 0)


def write_out(*refs):
    copies = [
        pltpu.make_async_copy(refs[i], refs[3 + i], refs[6].at[i]) for i in range(3)
    ]
    for copy in copies:
        copy.start()
    for copy in copies:
        copy.wait()


def on_device(n, n_fs, inputs, out_grad, pre_act, w_up, w_down_t):
    tok, d_model = inputs.shape
    group, cols = pre_act.shape
    shard = w_up.shape[0]
    chunks = max(1, shard // 128)
    factor = float(group * n) ** -0.5
    dma = pltpu.SemaphoreType.DMA
    vmem = pl.BlockSpec(memory_space=pltpu.VMEM)
    results = pl.pallas_call(
        functools.partial(kernel, n, n_fs, chunks, factor),
        out_shape=(
            pltpu.VMEM((tok, d_model), BF16),
            pltpu.VMEM((shard, cols), F32),
            pltpu.VMEM((shard, cols), F32),
        ),
        in_specs=[pl.BlockSpec(memory_space=pl.ANY)] * 5,
        out_specs=(vmem,) * 3,
        scratch_shapes=[
            pltpu.VMEM((2, group, d_model), BF16),
            pltpu.VMEM((2, n, shard, cols), BF16),
            pltpu.VMEM((2, group, cols), BF16),
            pltpu.VMEM((2, 2, n, shard, cols), BF16),
            pltpu.VMEM((n, 2, n_fs * tok, shard), BF16),
            pltpu.VMEM((n, n_fs * tok, shard), BF16),
            pltpu.VMEM((n, n_fs - 1, tok, shard), BF16),
            pltpu.VMEM((group, cols), BF16),
            dma((2,)),
            dma((2, chunks)),
            dma(()),
            dma(()),
        ],
        compiler_params=pltpu.CompilerParams(
            collective_id=0, has_side_effects=True, vmem_limit_bytes=56 * 2**20
        ),
    )(inputs, out_grad, pre_act, w_up, w_down_t)
    results = [pltpu.with_memory_space_constraint(a, pltpu.VMEM) for a in results]
    return pl.pallas_call(
        write_out,
        out_shape=[jax.ShapeDtypeStruct(a.shape, a.dtype) for a in results],
        in_specs=[vmem] * 3,
        out_specs=[pl.BlockSpec(memory_space=pl.ANY)] * 3,
        scratch_shapes=[dma((3,))],
        compiler_params=pltpu.CompilerParams(vmem_limit_bytes=2**20),
    )(*results)


def solution(mesh):
    rows = P(("rep", "fs", "tp"), None)
    blocks = P("rep", ("fs", "tp"))
    return jax.shard_map(
        functools.partial(on_device, mesh.shape["rep"], mesh.shape["fs"]),
        mesh=mesh,
        in_specs=(rows, rows, blocks, blocks, blocks),
        out_specs=(rows, blocks, blocks),
        check_vma=False,
    )
```
